512 devices in a mesh: sp: 64 (over z, y), tp: 8 (over x, core).
Axes of the slice: x: 4, y: 8, z: 8, core: 2. Of those that a mesh axis runs over, the one named last changes fastest.
Arguments:
- queries: bfloat16 [16384, 512], P('sp', 'tp'), may hold values from -8 to 8
- keys: bfloat16 [16384, 512], P('sp', 'tp'), may hold values from -8 to 8
- values: bfloat16 [16384, 512], P('sp', 'tp'), may hold values from -6 to 6
- score_shift: float32 [8], P('tp'), may hold values from 3 to 20
- resid: bfloat16 [16384, 2048], P(('sp', 'tp')), may hold values from -6 to 6
- w_out: bfloat16 [512, 2048], replicated, may hold values from -0.25 to 0.25
- gain_mix: float32 [2048], replicated, may hold values from 0.1 to 1.9
- gain_pre: float32 [2048], replicated, may hold values from 0.1 to 1.9
- w_gate: bfloat16 [2048, 5632], P('sp', 'tp'), may hold values from -0.125 to 0.125
- w_up: bfloat16 [2048, 5632], P('sp', 'tp'), may hold values from -0.125 to 0.125
- conv_gate: float32 [3, 5632], P(None, 'tp'), may hold values from -3 to 3
- conv_up: float32 [3, 5632], P(None, 'tp'), may hold values from -3 to 3
- w_down: bfloat16 [5632, 2048], P('tp', 'sp'), may hold values from -0.078125 to 0.078125
- gain_post: float32 [2048], replicated, may hold values from 0.1 to 1.9
Outputs:
- result: bfloat16 [16384, 2048], P(('sp', 'tp'))
The draws below stay inside these ranges and needn't reach their ends.
All inputs are finite; a program needn't handle non-finite values.
Results may differ from the reference program's by a relative error of at most 0.017.
Values may be sent and summed in bfloat16 or wider, within the bound.
A program may use at most 64 MiB of HBM per device.

```python
import math
import jax
import jax.numpy as jnp
from jax import lax

D = 2048
HEADS = 8
HEAD_DIM = 64
FF = 5632
KERNEL = 3
SEQ = 16384
N_TP = 8


def level_of(rng, dims, split, low, top_value):
    gain, own = 1.0, jax.random.fold_in(rng, 6)
    for axis_at, parts in split:
        heights = jnp.exp(jax.random.uniform(jax.random.fold_in(own, axis_at), (parts,), jnp.float32, low / len(split), top_value / len(split)))
        gain = gain * jnp.repeat(heights, dims[axis_at] // parts).reshape([-1 if axis == axis_at else 1 for axis in range(len(dims))])
    return gain


def scatter_about(key, dims, deviation, limit, shards=(), kind=jnp.bfloat16):
    factor_of = level_of(key, dims, shards, -0.22, 0.18) if shards else 1.0
    values = jax.random.normal(key, dims, jnp.float32) * deviation * factor_of
    return jnp.minimum(jnp.maximum(values, -limit), limit).astype(kind)


def setup_inputs(seed: int = 0) -> dict:
    arg_keys = jax.random.split(jax.random.key(seed), 15)
    queries = scatter_about(arg_keys[0], (SEQ, HEADS * HEAD_DIM), 2.0, 8.0, ((0, 64), (1, 8)))
    keys = scatter_about(arg_keys[1], (SEQ, HEADS * HEAD_DIM), 2.0, 8.0, ((0, 64), (1, 8)))
    values = scatter_about(arg_keys[2], (SEQ, HEADS * HEAD_DIM), 1.0, 6.0, ((0, 64), (1, 8)))
    score_shift = jnp.clip(jnp.exp(math.log(20.0) - 1.89712 * jax.random.uniform(arg_keys[3], (HEADS,), jnp.float32) ** level_of(arg_keys[3], (HEADS,), ((0, 8),), -0.2, 0.2)), 3.0, 20.0)
    resid = scatter_about(arg_keys[4], (SEQ, D), 1.0, 6.0, ((0, 512),))
    w_out = scatter_about(arg_keys[5], (HEADS * HEAD_DIM, D), (HEADS * HEAD_DIM) ** -0.5, 0.25)
    gain_mix = jnp.clip(1.0 + 0.18 * jax.random.normal(arg_keys[6], (D,), jnp.float32), 0.1, 1.9)
    gain_pre = jnp.clip(1.0 + 0.18 * jax.random.normal(arg_keys[7], (D,), jnp.float32), 0.1, 1.9)
    w_gate = scatter_about(arg_keys[8], (D, FF), D ** -0.5, 0.125, ((0, 64), (1, 8)))
    w_up = scatter_about(arg_keys[9], (D, FF), D ** -0.5, 0.125, ((0, 64), (1, 8)))
    conv_gate = scatter_about(arg_keys[10], (KERNEL, FF), 0.577, 3.0, ((1, 8),), jnp.float32)
    conv_up = scatter_about(arg_keys[11], (KERNEL, FF), 0.577, 3.0, ((1, 8),), jnp.float32)
    w_down = scatter_about(arg_keys[12], (FF, D), FF ** -0.5, 0.078125, ((0, 8), (1, 64)))
    gain_post = jnp.clip(1.0 + 0.18 * jax.random.normal(arg_keys[13], (D,), jnp.float32), 0.1, 1.9)
    return dict(queries=queries, keys=keys, values=values, score_shift=score_shift, resid=resid, w_out=w_out, gain_mix=gain_mix, gain_pre=gain_pre, w_gate=w_gate, w_up=w_up, conv_gate=conv_gate, conv_up=conv_up, w_down=w_down, gain_post=gain_post)


def rms_scale(values_in):
    return values_in * lax.rsqrt(lax.optimization_barrier(jnp.mean(values_in * values_in, axis=-1, keepdims=True)) + 1e-06)

def stick_attention(queries, keys, values, score_shift):
    length = queries.shape[0]
    query_heads = queries.reshape(length, HEADS, HEAD_DIM).transpose(1, 0, 2)
    key_heads = keys.reshape(length, HEADS, HEAD_DIM).transpose(1, 0, 2)
    value_heads = values.reshape(length, HEADS, HEAD_DIM).transpose(1, 0, 2)
    block = math.gcd(length, 512)
    blocks = length // block
    key_pos = jnp.arange(length, dtype=jnp.int32)

    def one_block(index):
        head = index // blocks
        first = index % blocks * block
        query_block = lax.dynamic_slice(query_heads, (head, first, jnp.int32(0)), (1, block, HEAD_DIM))[0]
        key_head = lax.dynamic_index_in_dim(key_heads, head, 0, keepdims=False)
        value_head = lax.dynamic_index_in_dim(value_heads, head, 0, keepdims=False)
        shift = lax.dynamic_index_in_dim(score_shift, head, 0, keepdims=False)
        scores = jnp.dot(query_block, key_head.T, preferred_element_type=jnp.float32) * HEAD_DIM ** (-0.5) - shift
        query_pos = first + jnp.arange(block, dtype=jnp.int32)
        causal = key_pos[None, :] < query_pos[:, None]
        log_keep = jnp.where(causal, -jax.nn.softplus(scores), 0.0)
        later = lax.cumsum(log_keep, axis=1, reverse=True) - log_keep
        weights = jnp.where(causal, jnp.exp(jax.nn.log_sigmoid(scores) + later), 0.0).astype(jnp.bfloat16)
        return jnp.dot(weights, value_head, preferred_element_type=jnp.float32).astype(jnp.bfloat16)
    outputs = lax.map(one_block, jnp.arange(HEADS * blocks, dtype=jnp.int32))
    outputs = outputs.reshape(HEADS, length, HEAD_DIM)
    return outputs.transpose(1, 0, 2).reshape(length, HEADS * HEAD_DIM)

def reference(queries, keys, values, score_shift, resid, w_out, gain_mix, gain_pre, w_gate, w_up, conv_gate, conv_up, w_down, gain_post):
    attended = stick_attention(queries, keys, values, score_shift)
    mixed = jnp.dot(attended, w_out, preferred_element_type=jnp.float32).astype(jnp.bfloat16)
    middle = (resid.astype(jnp.float32) + gain_mix * rms_scale(mixed.astype(jnp.float32))).astype(jnp.bfloat16)
    normed = (gain_pre * rms_scale(middle.astype(jnp.float32))).astype(jnp.bfloat16)
    gate_proj = jnp.dot(normed, w_gate, preferred_element_type=jnp.float32).astype(jnp.bfloat16)
    up_proj = jnp.dot(normed, w_up, preferred_element_type=jnp.float32).astype(jnp.bfloat16)
    length = normed.shape[0]
    gate_pad = jnp.pad(gate_proj.astype(jnp.float32), ((KERNEL - 1, 0), (0, 0)))
    up_pad = jnp.pad(up_proj.astype(jnp.float32), ((KERNEL - 1, 0), (0, 0)))
    gate_conv = jnp.zeros((length, FF), jnp.float32)
    up_conv = jnp.zeros((length, FF), jnp.float32)
    for tap in range(KERNEL):
        gate_conv = gate_conv + conv_gate[tap] * gate_pad[tap:tap + length]
        up_conv = up_conv + conv_up[tap] * up_pad[tap:tap + length]
    hidden = (jax.nn.silu(gate_conv) * up_conv).astype(jnp.bfloat16)
    width_block = FF // N_TP
    summed = jnp.zeros((length, D), jnp.float32)
    for index in range(N_TP):
        partial_sum = jnp.dot(hidden[:, index * width_block:(index + 1) * width_block], w_down[index * width_block:(index + 1) * width_block], preferred_element_type=jnp.float32)
        summed = summed + partial_sum.astype(jnp.bfloat16).astype(jnp.float32)
    ffn_out = summed.astype(jnp.bfloat16)
    return (middle.astype(jnp.float32) + gain_post * rms_scale(ffn_out.astype(jnp.float32))).astype(jnp.bfloat16)
```

```python
import functools
import math

import jax
import jax.numpy as jnp
from jax import lax
from jax.experimental import pallas as pl
from jax.experimental.pallas import tpu as pltpu
from jax.sharding import PartitionSpec as P

HEAD_DIM = 64
KERNEL = 3
RING = 8
MESH = pl.DeviceIdType.MESH
LOG2E = 1.0 / math.log(2.0)
LANES = 128


def from_everyone(x, axis):
    length = lax.axis_size(axis)
    return lax.all_to_all(jnp.broadcast_to(x[None], (length, *x.shape)), axis, 0, 0, tiled=True)


def from_behind(x, axis, by):
    length = lax.axis_size(axis)
    pairs = [(i, i + by) for i in range(length) if 0 <= i + by < length]
    return lax.ppermute(x, axis, pairs)


def sum_at_owner(x, axis):
    length = lax.axis_size(axis)
    parts = x.reshape(length, -1, x.shape[1])
    arrived = lax.all_to_all(parts, axis, split_axis=0, concat_axis=0, tiled=True)
    return arrived.astype(jnp.float32).sum(axis=0)


def rms_scale(values_in):
    return values_in * lax.rsqrt(jnp.mean(values_in * values_in, axis=-1, keepdims=True) + 1e-06)


def wrap(v):
    return lax.rem(v + 2 * RING, RING)


class Rings:
    def __init__(self, z, y, local, buf, send, recv, base):
        self.z, self.y, self.local, self.buf = z, y, local, buf
        self.send, self.recv, self.base = send, recv, base
        rows = local.shape[0]
        self.half = (pl.ds(0, rows // 2), pl.ds(rows // 2, rows // 2))
        self.copies = {}

    def _neighbour(self, along_y, sign):
        if along_y:
            return {"sp": self.z * RING + wrap(self.y + sign)}
        return {"sp": wrap(self.z + sign) * RING + self.y}

    def _start(self, key, src, dst, along_y, sign):
        slot = self.base + len(self.copies)
        copy = pltpu.make_async_remote_copy(
            src_ref=src,
            dst_ref=dst,
            send_sem=self.send.at[slot],
            recv_sem=self.recv.at[slot],
            device_id=self._neighbour(along_y, sign),
            device_id_type=MESH,
        )
        copy.start()
        self.copies[key] = copy

    def first(self, h, sign, s):
        rows = self.half[h]
        if h == 0:
            place = self.buf.at[self.z, wrap(self.y - sign * s), rows]
        else:
            place = self.buf.at[wrap(self.z - sign * s), self.y, rows]
        src = self.local.at[rows] if s == 0 else place
        self._start((1, h, sign, s), src, place, h == 0, sign)

    def second(self, h, sign, s, c):
        rows = self.half[h]
        chunk = pl.ds(c * (RING // 2), RING // 2)
        if h == 0:
            place = self.buf.at[wrap(self.z - sign * s), chunk, rows]
        else:
            place = self.buf.at[chunk, wrap(self.y - sign * s), rows]
        self._start((2, h, sign, s, c), place, place, h == 1, sign)

    def first_step(self, s):
        for h in (0, 1):
            for sign in (1, -1):
                if s > 0 and (1, h, sign, s - 1) in self.copies:
                    self.copies[(1, h, sign, s - 1)].wait_recv()
                if s < (4 if sign == 1 else 3):
                    self.first(h, sign, s)

    def second_step(self, s, c):
        for h in (0, 1):
            for sign in (1, -1):
                if s > 0 and (2, h, sign, s - 1, c) in self.copies:
                    self.copies[(2, h, sign, s - 1, c)].wait_recv()
                if s < 3 or (s == 3 and c == (0 if sign == 1 else 1)):
                    self.second(h, sign, s, c)

    def drain(self):
        for copy in self.copies.values():
            copy.wait_send()


UNITS = 14 + 28


def tile(q_ref, kv, tri, shift2, own):
    kvb = kv[...]
    raw = lax.dot_general(
        q_ref[...], kvb, (((1,), (1,)), ((), ())), preferred_element_type=jnp.float32
    )
    t = raw * (LOG2E * HEAD_DIM**-0.5) - shift2
    soft = jnp.log(1.0 + jnp.exp2(-jnp.abs(t))) * LOG2E
    keep = jnp.maximum(t, 0.0) + soft
    sig = jnp.minimum(t, 0.0) - soft
    if own:
        row = lax.broadcasted_iota(jnp.int32, t.shape, 0)
        col = lax.broadcasted_iota(jnp.int32, t.shape, 1)
        causal = col < row
        keep = jnp.where(causal, keep, 0.0)
    sums = jnp.dot(keep.astype(jnp.bfloat16), tri[...], preferred_element_type=jnp.float32)
    span = kvb.shape[0]
    weights = jnp.exp2(sig - sums[:, :span])
    if own:
        weights = jnp.where(causal, weights, 0.0)
    return jnp.dot(
        weights.astype(jnp.bfloat16), kvb, preferred_element_type=jnp.float32
    ), sums[:, span:]


def front_kernel(
    shift_ref, q_ref, kv_ref, w_ref, att_ref, wfull, kvbuf, tri, acc, tail, send, recv, here
):
    sp = lax.axis_index("sp")
    z, y = lax.div(sp, RING), lax.rem(sp, RING)
    barrier = pltpu.get_barrier_semaphore()
    for dz, dy in ((1, 0), (-1, 0), (0, 1), (0, -1)):
        pl.semaphore_signal(
            barrier,
            inc=1,
            device_id={"sp": wrap(z + dz) * RING + wrap(y + dy)},
            device_id_type=MESH,
        )
    pl.semaphore_wait(barrier, 4)

    kv = Rings(z, y, kv_ref, kvbuf, send, recv, 0)
    w = Rings(z, y, w_ref, wfull, send, recv, UNITS)
    own_kv = pltpu.make_async_copy(kv_ref, kvbuf.at[z, y], here.at[0])
    own_w = pltpu.make_async_copy(w_ref, wfull.at[z, y], here.at[1])
    kv.first_step(0)
    w.first_step(0)
    own_kv.start()
    own_w.start()
    span = kv_ref.shape[0]
    at = lax.broadcasted_iota(jnp.int32, tri.shape, 0)
    to = lax.broadcasted_iota(jnp.int32, tri.shape, 1)
    tri[...] = jnp.where((at > to) | (to >= span), 1.0, 0.0).astype(jnp.bfloat16)
    shift2 = shift_ref[0] * LOG2E
    first_out, first_tail = tile(q_ref, kv_ref, tri, shift2, True)
    acc[...] = first_out
    tail[...] = first_tail
    for s in range(1, 4):
        kv.first_step(s)
        w.first_step(s)
    kv.first_step(4)
    own_kv.wait()
    for c in (0, 1):
        kv.second_step(0, c)
    w.first_step(4)
    own_w.wait()
    for s in range(1, 4):
        for c in (0, 1):
            kv.second_step(s, c)
    for c in (0, 1):
        w.second_step(0, c)
    for c in (0, 1):
        kv.second_step(4, c)

    def visit(turn, carry):
        block = sp - turn
        out, total = tile(
            q_ref, kvbuf.at[lax.div(block, RING), lax.rem(block, RING)], tri, shift2, False
        )
        acc[...] += jnp.exp2(-tail[...]) * out
        tail[...] += total
        return carry

    def visits(low, high):
        lax.fori_loop(low, jnp.minimum(high, sp + 1), visit, 0)

    visits(1, 33)
    w.second_step(1, 0)
    visits(33, 65)
    w.second_step(1, 1)
    att_ref[...] = acc[:, HEAD_DIM:].astype(jnp.bfloat16)
    for s in (2, 3, 4):
        for c in (0, 1):
            w.second_step(s, c)
    kv.drain()
    w.drain()


def front(queries, keys, values, score_shift, packed):
    rows = queries.shape[0]
    wide = packed.shape[1]
    vmem = pl.BlockSpec(memory_space=pltpu.VMEM)
    return pl.pallas_call(
        front_kernel,
        out_shape=(
            jax.ShapeDtypeStruct((rows, HEAD_DIM), jnp.bfloat16),
            jax.ShapeDtypeStruct((RING, RING, packed.shape[0], wide), jnp.bfloat16),
        ),
        in_specs=[pl.BlockSpec(memory_space=pltpu.SMEM), vmem, vmem, vmem],
        out_specs=(vmem, vmem),
        scratch_shapes=[
            pltpu.VMEM((RING, RING, rows, LANES), jnp.bfloat16),
            pltpu.VMEM((rows, rows + LANES), jnp.bfloat16),
            pltpu.VMEM((rows, LANES), jnp.float32),
            pltpu.VMEM((rows, LANES), jnp.float32),
            pltpu.SemaphoreType.DMA((2 * UNITS,)),
            pltpu.SemaphoreType.DMA((2 * UNITS,)),
            pltpu.SemaphoreType.DMA((2,)),
        ],
        compiler_params=pltpu.CompilerParams(
            collective_id=0, has_side_effects=True, vmem_limit_bytes=48 * 1024 * 1024
        ),
        name="front",
    )(
        score_shift,
        jnp.pad(queries, ((0, 0), (0, LANES - HEAD_DIM))),
        jnp.concatenate([keys, values], axis=1),
        packed,
    )


def local(
    queries,
    keys,
    values,
    score_shift,
    resid,
    w_out,
    gain_mix,
    gain_pre,
    w_gate,
    w_up,
    conv_gate,
    conv_up,
    w_down,
    gain_post,
):
    units = w_gate.shape[1]
    pad = -(3 * units) % LANES
    packed = jnp.concatenate(
        [w_gate, w_up, w_down.T, jnp.zeros((w_gate.shape[0], pad), jnp.bfloat16)], axis=1
    )
    attended, whole = front(queries, keys, values, score_shift, packed)
    whole = whole.reshape(-1, packed.shape[1])
    head_rows = lax.all_to_all(attended, "tp", split_axis=0, concat_axis=1, tiled=True)
    mixed = jnp.dot(head_rows, w_out, preferred_element_type=jnp.float32).astype(jnp.bfloat16)
    middle = (resid.astype(jnp.float32) + gain_mix * rms_scale(mixed.astype(jnp.float32))).astype(
        jnp.bfloat16
    )
    normed = (gain_pre * rms_scale(middle.astype(jnp.float32))).astype(jnp.bfloat16)
    piece = from_everyone(normed, "tp").reshape(-1, normed.shape[1])
    projected = jnp.dot(
        piece, whole[:, : 2 * units], preferred_element_type=jnp.float32
    ).astype(jnp.bfloat16)
    tok_rows = projected.shape[0]
    edge = from_behind(projected[tok_rows - (KERNEL - 1) :], "sp", 1)
    extended = jnp.concatenate([edge, projected], axis=0).astype(jnp.float32)
    taps = jnp.concatenate([conv_gate, conv_up], axis=1)
    convolved = taps[0] * extended[0:tok_rows]
    for tap in range(1, KERNEL):
        convolved = convolved + taps[tap] * extended[tap : tap + tok_rows]
    hidden = (jax.nn.silu(convolved[:, :units]) * convolved[:, units:]).astype(jnp.bfloat16)
    partial = lax.dot_general(
        hidden,
        whole[:, 2 * units : 3 * units],
        (((1,), (1,)), ((), ())),
        preferred_element_type=jnp.float32,
    ).astype(jnp.bfloat16)
    ffn_out = sum_at_owner(partial, "tp").astype(jnp.bfloat16)
    return (middle.astype(jnp.float32) + gain_post * rms_scale(ffn_out.astype(jnp.float32))).astype(
        jnp.bfloat16
    )


def solution(mesh):
    in_specs = (
        P("sp", "tp"),
        P("sp", "tp"),
        P("sp", "tp"),
        P("tp"),
        P(("sp", "tp"), None),
        P(),
        P(),
        P(),
        P("sp", "tp"),
        P("sp", "tp"),
        P(None, "tp"),
        P(None, "tp"),
        P("tp", "sp"),
        P(),
    )
    out_specs = P(("sp", "tp"), None)
    return jax.shard_map(local, mesh=mesh, in_specs=in_specs, out_specs=out_specs, check_vma=False)
```

```python
import math

import jax
import jax.numpy as jnp
from jax import lax
from jax.experimental import pallas as pl
from jax.experimental.pallas import tpu as pltpu
from jax.sharding import PartitionSpec as P

HEAD_DIM = 64
KERNEL = 3
RING = 8
CHIPS = 4
GROUP = 8
MESH = pl.DeviceIdType.MESH
LOG2E = 1.0 / math.log(2.0)
LANES = 128
HALO = 16
UNROLL = 4
TRANSFERS = 256
LOADS = 8


def wrap(v, n):
    return lax.rem(v + 2 * n, n)


class Post:
    def __init__(self, send, recv):
        self.send, self.recv, self.copies = send, recv, []

    def start(self, src, dst, device):
        slot = len(self.copies)
        copy = pltpu.make_async_remote_copy(
            src_ref=src,
            dst_ref=dst,
            send_sem=self.send.at[slot],
            recv_sem=self.recv.at[slot],
            device_id=device,
            device_id_type=MESH,
        )
        copy.start()
        self.copies.append(copy)
        return copy

    def drain(self):
        for copy in self.copies:
            copy.wait_send()


class Rings:
    def __init__(self, post, z, y, buf):
        self.post, self.z, self.y, self.buf = post, z, y, buf
        rows = buf.shape[2]
        self.half = (pl.ds(0, rows // 2), pl.ds(rows // 2, rows // 2))
        self.copies = {}

    def _neighbour(self, along_y, sign):
        if along_y:
            return {"sp": self.z * RING + wrap(self.y + sign, RING)}
        return {"sp": wrap(self.z + sign, RING) * RING + self.y}

    def first(self, h, sign, s):
        rows = self.half[h]
        if h == 0:
            place = self.buf.at[self.z, wrap(self.y - sign * s, RING), rows]
        else:
            place = self.buf.at[wrap(self.z - sign * s, RING), self.y, rows]
        self.copies[(1, h, sign, s)] = self.post.start(place, place, self._neighbour(h == 0, sign))

    def second(self, h, sign, s, c):
        rows = self.half[h]
        chunk = pl.ds(c * (RING // 2), RING // 2)
        if h == 0:
            place = self.buf.at[wrap(self.z - sign * s, RING), chunk, rows]
        else:
            place = self.buf.at[chunk, wrap(self.y - sign * s, RING), rows]
        self.copies[(2, h, sign, s, c)] = self.post.start(
            place, place, self._neighbour(h == 1, sign)
        )

    def first_step(self, s):
        for h in (0, 1):
            for sign in (1, -1):
                if (1, h, sign, s - 1) in self.copies:
                    self.copies[(1, h, sign, s - 1)].wait_recv()
                if s < (4 if sign == 1 else 3):
                    self.first(h, sign, s)

    def second_step(self, s, c):
        for h in (0, 1):
            for sign in (1, -1):
                if (2, h, sign, s - 1, c) in self.copies:
                    self.copies[(2, h, sign, s - 1, c)].wait_recv()
                if s < 3 or (s == 3 and c == (0 if sign == 1 else 1)):
                    self.second(h, sign, s, c)


def tile(query, pair, tri, shift2, own):
    raw = jnp.dot(query, pair, preferred_element_type=jnp.float32)
    t = raw * (LOG2E * HEAD_DIM**-0.5) - shift2
    spent = jnp.maximum(t, jnp.log(1.0 + jnp.exp2(jnp.minimum(t, 126.0))) * LOG2E)
    taken = t - spent
    if own:
        row = lax.broadcasted_iota(jnp.int32, t.shape, 0)
        col = lax.broadcasted_iota(jnp.int32, t.shape, 1)
        causal = col < row
        spent = jnp.where(causal, spent, 0.0)
    later = jnp.dot(spent.astype(jnp.bfloat16), tri, preferred_element_type=jnp.float32)
    weights = jnp.exp2(taken - later)
    if own:
        weights = jnp.where(causal, weights, 0.0)
    total = jnp.broadcast_to(later[:, :1] + spent[:, :1], (t.shape[0], LANES))
    out = lax.dot_general(
        weights.astype(jnp.bfloat16),
        pair,
        (((1,), (1,)), ((), ())),
        preferred_element_type=jnp.float32,
    )
    return out, total


def rms_scale(v):
    return v * lax.rsqrt(jnp.mean(v * v, axis=-1, keepdims=True) + 1e-06)


def rounded(v):
    return v.astype(jnp.bfloat16).astype(jnp.float32)


def layer_kernel(
    shift_ref,
    gain_mix,
    gain_pre,
    gain_post,
    conv_gate,
    conv_up,
    q_hbm,
    k_hbm,
    v_hbm,
    gate_hbm,
    up_hbm,
    down_hbm,
    resid_hbm,
    wout_hbm,
    result,
    qt,
    query,
    pairs,
    gate,
    up,
    down,
    whole,
    resid,
    wout,
    tri,
    acc,
    tail,
    attended,
    arrived,
    piece,
    middle,
    edge_out,
    edge_in,
    extended,
    hidden,
    partial,
    partner_partial,
    summed,
    landed,
    passed,
    send,
    recv,
    load,
    edge_sem,
):
    sp, tp = lax.axis_index("sp"), lax.axis_index("tp")
    z, y = lax.div(sp, RING), lax.rem(sp, RING)
    x, core = lax.div(tp, 2), lax.rem(tp, 2)
    shards = RING * RING
    span = query.shape[0]
    own_rows = result.shape[0]
    width = gate.shape[1]
    mains = width // LANES
    rest = width - mains * LANES

    loads = [
        pltpu.make_async_copy(a, b, load.at[i])
        for i, (a, b) in enumerate(
            (
                (k_hbm, pairs.at[z, y, pl.ds(0, HEAD_DIM)]),
                (v_hbm, pairs.at[z, y, pl.ds(HEAD_DIM, HEAD_DIM)]),
                (gate_hbm, gate),
                (up_hbm, up),
                (down_hbm, down),
                (q_hbm, qt),
                (resid_hbm, resid),
                (wout_hbm, wout),
            )
        )
    ]
    for copy in loads:
        copy.start()
    barrier = pltpu.get_barrier_semaphore()
    greeted = [
        {"sp": wrap(z + dz, RING) * RING + wrap(y + dy, RING)}
        for dz, dy in ((1, 0), (-1, 0), (0, 1), (0, -1))
    ]
    greeted += [{"sp": wrap(sp + 1, shards)}, {"sp": wrap(sp - 1, shards)}]
    greeted += [{"tp": wrap(tp + k, GROUP)} for k in range(1, GROUP)]
    for device in greeted:
        pl.semaphore_signal(barrier, inc=1, device_id=device, device_id_type=MESH)
    for copy in loads[2:5]:
        copy.wait()
    for j in range(mains):
        here = slice(j * LANES, (j + 1) * LANES)
        whole[z, y, :, 2 * j * LANES : (2 * j + 1) * LANES] = gate[:, here]
        whole[z, y, :, (2 * j + 1) * LANES : (2 * j + 2) * LANES] = up[:, here]
    base = 2 * mains * LANES
    whole[z, y, :, base : base + LANES] = jnp.concatenate(
        [gate[:, mains * LANES :], up[:, mains * LANES :]], axis=1
    )
    down_at = base + LANES
    whole[z, y, :, down_at : down_at + mains * LANES] = down[:, : mains * LANES]
    whole[z, y, :, down_at + mains * LANES :] = jnp.concatenate(
        [down[:, mains * LANES :], jnp.zeros((down.shape[0], LANES - rest), jnp.bfloat16)], axis=1
    )
    for copy in loads[:2]:
        copy.wait()
    pl.semaphore_wait(barrier, len(greeted))

    post = Post(send, recv)
    kv = Rings(post, z, y, pairs)
    w = Rings(post, z, y, whole)
    kv.first_step(0)
    w.first_step(0)

    at = lax.broadcasted_iota(jnp.int32, tri.shape, 0)
    to = lax.broadcasted_iota(jnp.int32, tri.shape, 1)
    tri[...] = jnp.where(at > to, 1.0, 0.0).astype(jnp.bfloat16)
    loads[5].wait()
    padded = jnp.concatenate(
        [qt[...].astype(jnp.float32), jnp.zeros(qt.shape, jnp.float32)], axis=0
    )
    query[...] = padded.T.astype(jnp.bfloat16)
    shift2 = shift_ref[0] * LOG2E
    kv.first_step(1)
    w.first_step(1)
    first_out, first_tail = tile(query[...], pairs[z, y], tri[...], shift2, True)
    acc[...] = first_out
    tail[...] = first_tail
    for s in (2, 3):
        kv.first_step(s)
        w.first_step(s)
    kv.first_step(4)
    for c in (0, 1):
        kv.second_step(0, c)
    w.first_step(4)
    for s in (1, 2, 3):
        for c in (0, 1):
            kv.second_step(s, c)
    for c in (0, 1):
        w.second_step(0, c)
    for c in (0, 1):
        kv.second_step(4, c)

    def visit(first, count):
        found = []
        for k in range(count):
            block = sp - first - k
            pair = pairs[lax.div(block, RING), lax.rem(block, RING)]
            found.append(tile(query[...], pair, tri[...], shift2, False))
        total, spent = acc[...], tail[...]
        for out, more in found:
            total = total + jnp.exp2(-spent) * out
            spent = spent + more
        acc[...] = total
        tail[...] = spent

    odd = lax.rem(sp, UNROLL)
    many = lax.div(sp, UNROLL)

    def one(turn, carry):
        visit(turn + 1, 1)
        return carry

    def several(turn, carry):
        visit(1 + odd + turn * UNROLL, UNROLL)
        return carry

    lax.fori_loop(0, odd, one, 0)
    lax.fori_loop(0, jnp.minimum(many, 6), several, 0)
    w.second_step(1, 0)
    lax.fori_loop(6, jnp.minimum(many, 11), several, 0)
    w.second_step(1, 1)
    lax.fori_loop(11, many, several, 0)

    lane = lax.broadcasted_iota(jnp.int32, acc.shape, 1)
    mine = lax.div(lane, HEAD_DIM) == core
    turned = jnp.where(core == 0, pltpu.roll(acc[...], HEAD_DIM, axis=1), acc[...])
    attended[...] = jnp.where(mine, turned, 0.0).astype(jnp.bfloat16)
    exchange = []
    for k in range(1, GROUP):
        peer = wrap(tp + k, GROUP)
        rows = pl.ds(pl.multiple_of(peer * own_rows, own_rows), own_rows)
        exchange.append(post.start(attended.at[rows], arrived.at[tp], {"tp": peer}))
    arrived[tp] = attended[pl.ds(pl.multiple_of(tp * own_rows, own_rows), own_rows), :]
    w.second_step(2, 0)
    loads[6].wait()
    loads[7].wait()
    for copy in exchange:
        copy.wait_recv()
    heads = jnp.concatenate([arrived[2 * i] + arrived[2 * i + 1] for i in range(CHIPS)], axis=1)
    mixed = rounded(jnp.dot(heads, wout[...], preferred_element_type=jnp.float32))
    mid = rounded(resid[...].astype(jnp.float32) + gain_mix[...] * rms_scale(mixed))
    middle[...] = mid
    normed = rounded(gain_pre[...] * rms_scale(mid))

    right, left = wrap(x + 1, CHIPS), wrap(x - 1, CHIPS)

    def rows_of(chip, c, half=None):
        start = HALO + (2 * chip + c) * own_rows
        if half is None:
            return piece.at[pl.ds(pl.multiple_of(start, HALO), own_rows)]
        start = start + half * (own_rows // 2)
        return piece.at[pl.ds(pl.multiple_of(start, HALO), own_rows // 2)]

    def to_chip(chip):
        return {"tp": 2 * chip + core}

    partner = {"tp": 2 * x + 1 - core}

    def move(ref, device):
        return post.start(ref, ref, device)

    piece[pl.ds(pl.multiple_of(HALO + tp * own_rows, HALO), own_rows), :] = normed.astype(
        jnp.bfloat16
    )
    edge_out[...] = normed[own_rows - (KERNEL - 1) :, :]
    plus = [move(rows_of(x, core, 0), to_chip(right))]
    minus = [move(rows_of(x, core, 1), to_chip(left))]
    plus.append(move(rows_of(x, core, 1), to_chip(right)))
    minus.append(move(rows_of(x, core, 0), to_chip(left)))
    across = [move(rows_of(x, core), partner)]

    def edge_copy(src, device, slot):
        return pltpu.make_async_remote_copy(
            src_ref=src,
            dst_ref=edge_in,
            send_sem=edge_sem.at[slot],
            recv_sem=edge_sem.at[GROUP],
            device_id=device,
            device_id_type=MESH,
        )

    last = tp == GROUP - 1
    ahead = edge_copy(edge_out, {"sp": wrap(sp + 1, shards)}, 0)

    @pl.when(last & (sp < shards - 1))
    def _():
        ahead.start()

    w.second_step(2, 1)
    plus[0].wait_recv()
    plus.append(move(rows_of(left, core, 0), to_chip(right)))
    across.append(move(rows_of(left, core, 0), partner))
    minus[0].wait_recv()
    minus.append(move(rows_of(right, core, 1), to_chip(left)))
    across.append(move(rows_of(right, core, 1), partner))
    plus[1].wait_recv()
    across.append(move(rows_of(left, core, 1), partner))
    minus[1].wait_recv()
    across.append(move(rows_of(right, core, 0), partner))
    far = wrap(x + 2, CHIPS)
    plus[2].wait_recv()
    across.append(move(rows_of(far, core, 0), partner))
    minus[2].wait_recv()
    across.append(move(rows_of(far, core, 1), partner))
    w.second_step(3, 0)

    spread = [edge_copy(edge_in, {"tp": wrap(tp + k, GROUP)}, k) for k in range(1, GROUP)]

    @pl.when(sp > 0)
    def _():
        spread[0].wait_recv()

        @pl.when(last)
        def _():
            for copy in spread:
                copy.start()

    behind = edge_in[...]
    place = lax.broadcasted_iota(jnp.int32, (HALO, piece.shape[1]), 0)
    front = jnp.where(sp > 0, 1, 0)
    filled = jnp.where(
        (place == HALO - 1) & (front == 1),
        behind[1:2, :],
        jnp.where((place == HALO - 2) & (front == 1), behind[0:1, :], 0.0),
    )
    piece[0:HALO, :] = filled.astype(jnp.bfloat16)
    for copy in across:
        copy.wait_recv()
    w.second_step(3, 1)
    w.second_step(4, 0)
    w.second_step(4, 1)

    depth = piece.shape[1]

    def convolve(low, high, taps):
        rows = partial.shape[0] * own_rows
        found = 0.0
        for tap in range(KERNEL):
            found = found + taps[tap : tap + 1, :] * extended[
                pl.ds(HALO - KERNEL + 1 + tap, rows), low:high
            ]
        return found

    def silu(v):
        return v / (1.0 + jnp.exp(-v))

    for j in range(mains):
        cols = slice(2 * j * LANES, (2 * j + 2) * LANES)
        rhs = whole[:, :, :, cols].reshape(depth, 2 * LANES)
        extended[...] = rounded(jnp.dot(piece[...], rhs, preferred_element_type=jnp.float32))
        here = slice(j * LANES, (j + 1) * LANES)
        g = convolve(0, LANES, conv_gate[:, here])
        u = convolve(LANES, 2 * LANES, conv_up[:, here])
        hidden[:, here] = (silu(g) * u).astype(jnp.bfloat16)
    rhs = whole[:, :, :, base : base + LANES].reshape(depth, LANES)
    extended[:, :LANES] = rounded(jnp.dot(piece[...], rhs, preferred_element_type=jnp.float32))
    taps = jnp.concatenate([conv_gate[:, mains * LANES :], conv_up[:, mains * LANES :]], axis=1)
    both = convolve(0, LANES, taps)
    product = silu(both) * pltpu.roll(both, LANES - rest, axis=1)
    inside = lax.broadcasted_iota(jnp.int32, product.shape, 1) < rest
    hidden[:, mains * LANES :] = jnp.where(inside, product, 0.0).astype(jnp.bfloat16)

    for j in range(RING):
        rhs = whole[j, :, :, down_at:].reshape(depth // RING, hidden.shape[1])
        found = lax.dot_general(
            hidden[...], rhs, (((1,), (1,)), ((), ())), preferred_element_type=jnp.float32
        )
        partial[:, :, j * (depth // RING) : (j + 1) * (depth // RING)] = found.astype(
            jnp.bfloat16
        ).reshape(partial.shape[0], own_rows, depth // RING)

    swaps = [
        post.start(partial.at[2 * chip + 1 - core], partner_partial.at[chip], partner)
        for chip in range(CHIPS)
    ]
    halves = (pl.ds(0, own_rows // 2), pl.ds(own_rows // 2, own_rows // 2))
    for copy in swaps:
        copy.wait_recv()
    for chip in range(CHIPS):
        summed[chip] = (
            partial[2 * chip + core].astype(jnp.float32)
            + partner_partial[chip].astype(jnp.float32)
        ).astype(jnp.bfloat16)

    def give(src, slot, chip):
        return post.start(src, landed.at[slot], to_chip(chip))

    got = [
        give(summed.at[far, halves[0]], 0, right),
        give(summed.at[far, halves[1]], 1, left),
        give(summed.at[right, halves[1]], 2, right),
        give(summed.at[left, halves[0]], 3, left),
    ]
    got[0].wait_recv()
    passed[0] = (
        summed[right, halves[0], :].astype(jnp.float32) + landed[0].astype(jnp.float32)
    ).astype(jnp.bfloat16)
    got.append(give(passed.at[0], 4, right))
    got[1].wait_recv()
    passed[1] = (
        summed[left, halves[1], :].astype(jnp.float32) + landed[1].astype(jnp.float32)
    ).astype(jnp.bfloat16)
    got.append(give(passed.at[1], 5, left))
    for copy in got[2:]:
        copy.wait_recv()
    for h, (near, through) in enumerate(((3, 4), (2, 5))):
        ffn = rounded(
            summed[x, halves[h], :].astype(jnp.float32)
            + landed[near].astype(jnp.float32)
            + landed[through].astype(jnp.float32)
        )
        result[halves[h], :] = (
            middle[halves[h], :] + gain_post[...] * rms_scale(ffn)
        ).astype(jnp.bfloat16)

    post.drain()

    @pl.when(last & (sp < shards - 1))
    def _():
        ahead.wait_send()

    @pl.when(last & (sp > 0))
    def _():
        for copy in spread:
            copy.wait_send()


def local(
    queries,
    keys,
    values,
    score_shift,
    resid,
    w_out,
    gain_mix,
    gain_pre,
    w_gate,
    w_up,
    conv_gate,
    conv_up,
    w_down,
    gain_post,
):
    span = queries.shape[0]
    own_rows, depth = resid.shape
    width = w_gate.shape[1]
    mains = width // LANES
    slab = w_gate.shape[0]
    columns = 2 * mains * LANES + LANES + (mains + 1) * LANES
    vmem = pl.BlockSpec(memory_space=pltpu.VMEM)
    anywhere = pl.BlockSpec(memory_space=pl.ANY)
    bf16, f32 = jnp.bfloat16, jnp.float32
    return pl.pallas_call(
        layer_kernel,
        out_shape=jax.ShapeDtypeStruct((own_rows, depth), bf16),
        in_specs=[pl.BlockSpec(memory_space=pltpu.SMEM)] + [vmem] * 5 + [anywhere] * 8,
        out_specs=vmem,
        scratch_shapes=[
            pltpu.VMEM((HEAD_DIM, span), bf16),
            pltpu.VMEM((span, LANES), bf16),
            pltpu.VMEM((RING, RING, 2 * HEAD_DIM, span), bf16),
            pltpu.VMEM((slab, width), bf16),
            pltpu.VMEM((slab, width), bf16),
            pltpu.VMEM((slab, width), bf16),
            pltpu.VMEM((RING, RING, slab, columns), bf16),
            pltpu.VMEM((own_rows, depth), bf16),
            pltpu.VMEM(w_out.shape, bf16),
            pltpu.VMEM((span, span), bf16),
            pltpu.VMEM((span, LANES), f32),
            pltpu.VMEM((span, LANES), f32),
            pltpu.VMEM((span, LANES), bf16),
            pltpu.VMEM((GROUP, own_rows, LANES), bf16),
            pltpu.VMEM((HALO + span, depth), bf16),
            pltpu.VMEM((own_rows, depth), f32),
            pltpu.VMEM((KERNEL - 1, depth), f32),
            pltpu.VMEM((KERNEL - 1, depth), f32),
            pltpu.VMEM((HALO + span, 2 * LANES), f32),
            pltpu.VMEM((span, (mains + 1) * LANES), bf16),
            pltpu.VMEM((GROUP, own_rows, depth), bf16),
            pltpu.VMEM((CHIPS, own_rows, depth), bf16),
            pltpu.VMEM((CHIPS, own_rows, depth), bf16),
            pltpu.VMEM((6, own_rows // 2, depth), bf16),
            pltpu.VMEM((2, own_rows // 2, depth), bf16),
            pltpu.SemaphoreType.DMA((TRANSFERS,)),
            pltpu.SemaphoreType.DMA((TRANSFERS,)),
            pltpu.SemaphoreType.DMA((LOADS,)),
            pltpu.SemaphoreType.DMA((GROUP + 1,)),
        ],
        compiler_params=pltpu.CompilerParams(
            collective_id=0, has_side_effects=True, vmem_limit_bytes=52 * 1024 * 1024
        ),
        name="layer",
    )(
        score_shift,
        gain_mix[None],
        gain_pre[None],
        gain_post[None],
        conv_gate,
        conv_up,
        queries.T,
        keys.T,
        values.T,
        w_gate,
        w_up,
        w_down.T,
        resid,
        w_out,
    )


def solution(mesh):
    in_specs = (
        P("sp", "tp"),
        P("sp", "tp"),
        P("sp", "tp"),
        P("tp"),
        P(("sp", "tp"), None),
        P(),
        P(),
        P(),
        P("sp", "tp"),
        P("sp", "tp"),
        P(None, "tp"),
        P(None, "tp"),
        P("tp", "sp"),
        P(),
    )
    out_specs = P(("sp", "tp"), None)
    return jax.shard_map(local, mesh=mesh, in_specs=in_specs, out_specs=out_specs, check_vma=False)
```

```python
import math

import jax
import jax.numpy as jnp
from jax import lax
from jax.experimental import pallas as pl
from jax.experimental.pallas import tpu as pltpu
from jax.sharding import PartitionSpec as P

HEAD_DIM = 64
KERNEL = 3
RING = 8
CHIPS = 4
GROUP = 8
MESH = pl.DeviceIdType.MESH
LOG2E = 1.0 / math.log(2.0)
LANES = 128
HALO = 16
UNROLL = 4
TRANSFERS = 256
LOADS = 14


def wrap(v, n):
    return lax.rem(v + 2 * n, n)


class Post:
    def __init__(self, send, recv):
        self.send, self.recv, self.copies = send, recv, []

    def start(self, src, dst, device):
        slot = len(self.copies)
        copy = pltpu.make_async_remote_copy(
            src_ref=src,
            dst_ref=dst,
            send_sem=self.send.at[slot],
            recv_sem=self.recv.at[slot],
            device_id=device,
            device_id_type=MESH,
        )
        copy.start()
        self.copies.append(copy)
        return copy

    def drain(self):
        for copy in self.copies:
            copy.wait_send()


class Line:
    def __init__(self, post, me, place, device):
        self.post, self.me, self.place, self.device = post, me, place, device
        self.copies = {}

    def step(self, s):
        for sign in (1, -1):
            if (sign, s - 1) in self.copies:
                self.copies[(sign, s - 1)].wait_recv()
            if s < RING // 2:
                part = None if s < RING // 2 - 1 else (0 if sign == 1 else 1)
                ref = self.place(wrap(self.me - sign * s, RING), part)
                self.copies[(sign, s)] = self.post.start(
                    ref, ref, self.device(wrap(self.me + sign, RING))
                )


class Rings:
    def __init__(self, post, z, y, buf):
        self.post, self.z, self.y, self.buf = post, z, y, buf
        rows = buf.shape[2]
        self.half = (pl.ds(0, rows // 2), pl.ds(rows // 2, rows // 2))
        self.copies = {}

    def _neighbour(self, along_y, sign):
        if along_y:
            return {"sp": self.z * RING + wrap(self.y + sign, RING)}
        return {"sp": wrap(self.z + sign, RING) * RING + self.y}

    def first(self, h, sign, s):
        rows = self.half[h]
        if h == 0:
            place = self.buf.at[self.z, wrap(self.y - sign * s, RING), rows]
        else:
            place = self.buf.at[wrap(self.z - sign * s, RING), self.y, rows]
        self.copies[(1, h, sign, s)] = self.post.start(place, place, self._neighbour(h == 0, sign))

    def second(self, h, sign, s, c):
        rows = self.half[h]
        chunk = pl.ds(c * (RING // 2), RING // 2)
        if h == 0:
            place = self.buf.at[wrap(self.z - sign * s, RING), chunk, rows]
        else:
            place = self.buf.at[chunk, wrap(self.y - sign * s, RING), rows]
        self.copies[(2, h, sign, s, c)] = self.post.start(
            place, place, self._neighbour(h == 1, sign)
        )

    def carries(self, h, sign, c):
        return sign == -1 if h == 0 else c == (0 if sign == 1 else 1)

    def first_step(self, s):
        for h in (0, 1):
            for sign in (1, -1):
                if (1, h, sign, s - 1) in self.copies:
                    self.copies[(1, h, sign, s - 1)].wait_recv()
                if s < (4 if sign == 1 else 3):
                    self.first(h, sign, s)

    def second_step(self, s, c):
        for h in (0, 1):
            for sign in (1, -1):
                if (2, h, sign, s - 1, c) in self.copies:
                    self.copies[(2, h, sign, s - 1, c)].wait_recv()
                if s < 3 or (s == 3 and self.carries(h, sign, c)):
                    self.second(h, sign, s, c)


def tile(query, pair, tri, shift2, own):
    raw = jnp.dot(query, pair, preferred_element_type=jnp.float32)
    t = raw * (LOG2E * HEAD_DIM**-0.5) - shift2
    spent = jnp.maximum(t, jnp.log(1.0 + jnp.exp2(jnp.minimum(t, 126.0))) * LOG2E)
    taken = t - spent
    if own:
        row = lax.broadcasted_iota(jnp.int32, t.shape, 0)
        col = lax.broadcasted_iota(jnp.int32, t.shape, 1)
        causal = col < row
        spent = jnp.where(causal, spent, 0.0)
    later = jnp.dot(spent.astype(jnp.bfloat16), tri, preferred_element_type=jnp.float32)
    weights = jnp.exp2(taken - later)
    if own:
        weights = jnp.where(causal, weights, 0.0)
    total = jnp.broadcast_to(later[:, :1] + spent[:, :1], (t.shape[0], LANES))
    out = lax.dot_general(
        weights.astype(jnp.bfloat16),
        pair,
        (((1,), (1,)), ((), ())),
        preferred_element_type=jnp.float32,
    )
    return out, total


def rms_scale(v):
    return v * lax.rsqrt(jnp.mean(v * v, axis=-1, keepdims=True) + 1e-06)


def rounded(v):
    return v.astype(jnp.bfloat16).astype(jnp.float32)


def layer_kernel(
    shift_hbm,
    mix_hbm,
    pre_hbm,
    post_hbm,
    conv_gate_hbm,
    conv_up_hbm,
    q_hbm,
    k_hbm,
    v_hbm,
    gate_hbm,
    up_hbm,
    down_hbm,
    resid_hbm,
    wout_hbm,
    result,
    shift_ref,
    gain_mix,
    gain_pre,
    gain_post,
    conv_gate,
    conv_up,
    queries,
    query,
    pairs,
    gate,
    up,
    down,
    whole,
    resid,
    wout,
    tri,
    acc,
    tail,
    attended,
    messages,
    returned,
    mine,
    arrived,
    piece,
    middle,
    edge_out,
    edge_in,
    extended,
    hidden,
    partial,
    partner_partial,
    summed,
    landed,
    passed,
    send,
    recv,
    load,
    edge_sem,
    give_sem,
    take_sem,
):
    sp, tp = lax.axis_index("sp"), lax.axis_index("tp")
    z, y = lax.div(sp, RING), lax.rem(sp, RING)
    x, core = lax.div(tp, 2), lax.rem(tp, 2)
    shards = RING * RING
    span = query.shape[0]
    own_rows = result.shape[0]
    width = gate.shape[1]
    mains = width // LANES
    rest = width - mains * LANES

    loads = [
        pltpu.make_async_copy(a, b, load.at[i])
        for i, (a, b) in enumerate(
            (
                (k_hbm, pairs.at[y, pl.ds(0, HEAD_DIM)]),
                (v_hbm, pairs.at[y, pl.ds(HEAD_DIM, HEAD_DIM)]),
                (q_hbm, queries.at[z]),
                (gate_hbm, gate),
                (up_hbm, up),
                (down_hbm, down),
                (shift_hbm, shift_ref),
                (resid_hbm, resid),
                (wout_hbm, wout),
                (mix_hbm, gain_mix),
                (pre_hbm, gain_pre),
                (post_hbm, gain_post),
                (conv_gate_hbm, conv_gate),
                (conv_up_hbm, conv_up),
            )
        )
    ]
    for copy in loads:
        copy.start()
    barrier = pltpu.get_barrier_semaphore()
    greeted = [{"sp": z * RING + wrap(y + k, RING)} for k in (1, -1)]
    greeted += [{"sp": wrap(z + k, RING) * RING + y} for k in range(1, RING)]
    greeted += [{"sp": wrap(sp + 1, shards)}, {"sp": wrap(sp - 1, shards)}]
    greeted += [{"tp": wrap(tp + k, GROUP)} for k in range(1, GROUP)]
    for device in greeted:
        pl.semaphore_signal(barrier, inc=1, device_id=device, device_id_type=MESH)
    for copy in loads[3:6]:
        copy.wait()
    for j in range(mains):
        here = slice(j * LANES, (j + 1) * LANES)
        whole[z, y, :, 2 * j * LANES : (2 * j + 1) * LANES] = gate[:, here]
        whole[z, y, :, (2 * j + 1) * LANES : (2 * j + 2) * LANES] = up[:, here]
    base = 2 * mains * LANES
    whole[z, y, :, base : base + LANES] = jnp.concatenate(
        [gate[:, mains * LANES :], up[:, mains * LANES :]], axis=1
    )
    down_at = base + LANES
    whole[z, y, :, down_at : down_at + mains * LANES] = down[:, : mains * LANES]
    whole[z, y, :, down_at + mains * LANES :] = jnp.concatenate(
        [down[:, mains * LANES :], jnp.zeros((down.shape[0], LANES - rest), jnp.bfloat16)], axis=1
    )
    for copy in loads[:3]:
        copy.wait()
    pl.semaphore_wait(barrier, len(greeted))

    post = Post(send, recv)

    def key_place(i, part):
        return pairs.at[i] if part is None else pairs.at[i, pl.ds(part * HEAD_DIM, HEAD_DIM)]

    def query_place(i, part):
        half = HEAD_DIM // 2
        return queries.at[i] if part is None else queries.at[i, pl.ds(part * half, half)]

    kv = Line(post, y, key_place, lambda i: {"sp": z * RING + i})
    qs = Line(post, z, query_place, lambda i: {"sp": i * RING + y})
    w = Rings(post, z, y, whole)
    kv.step(0)
    qs.step(0)
    w.first_step(0)

    at = lax.broadcasted_iota(jnp.int32, tri.shape, 0)
    to = lax.broadcasted_iota(jnp.int32, tri.shape, 1)
    tri[...] = jnp.where(at > to, 1.0, 0.0).astype(jnp.bfloat16)
    loads[6].wait()
    shift2 = shift_ref[0] * LOG2E

    def set_query(i):
        padded = jnp.concatenate(
            [queries[i].astype(jnp.float32), jnp.zeros(queries.shape[1:], jnp.float32)], axis=0
        )
        query[...] = padded.T.astype(jnp.bfloat16)

    def visit(first, count, fresh=False):
        found = [
            tile(query[...], pairs[first - k], tri[...], shift2, False) for k in range(count)
        ]
        if fresh:
            total, spent = found.pop(0)
        else:
            total, spent = acc[...], tail[...]
        for out, more in found:
            total = total + jnp.exp2(-spent) * out
            spent = spent + more
        acc[...] = total
        tail[...] = spent

    def report():
        lane = lax.broadcasted_iota(jnp.int32, acc.shape, 1)
        return jnp.where(lane < HEAD_DIM, tail[...], acc[...]).T

    kv.step(1)
    qs.step(1)
    w.first_step(1)
    set_query(z)
    first_out, first_tail = tile(query[...], pairs[y], tri[...], shift2, True)
    acc[...] = first_out
    tail[...] = first_tail
    for s in (2, 3):
        kv.step(s)
        qs.step(s)
        w.first_step(s)
    kv.step(4)
    qs.step(4)
    w.first_step(4)
    for c in (0, 1):
        w.second_step(0, c)

    def one(turn, carry):
        visit(y - 1 - turn, 1)
        return carry

    def several(turn, carry):
        visit(y - 1 - lax.rem(y, UNROLL) - turn * UNROLL, UNROLL)
        return carry

    lax.fori_loop(0, lax.rem(y, UNROLL), one, 0)
    lax.fori_loop(0, lax.div(y, UNROLL), several, 0)
    mine[...] = report()

    def result_copy(i, there):
        return pltpu.make_async_remote_copy(
            src_ref=messages.at[i],
            dst_ref=returned.at[there],
            send_sem=give_sem.at[i],
            recv_sem=take_sem.at[there],
            device_id={"sp": i * RING + y},
            device_id_type=MESH,
        )

    def serve(turn, carry):
        i = z + 1 + turn
        set_query(i)
        visit(RING - 1, UNROLL, fresh=True)
        visit(RING - 1 - UNROLL, UNROLL)
        found = report()
        spent = found[: HEAD_DIM // 8, :]
        high = spent.astype(jnp.bfloat16)
        low = (spent - high.astype(jnp.float32)).astype(jnp.bfloat16)
        messages[i] = jnp.concatenate(
            [found[HEAD_DIM:, :].astype(jnp.bfloat16), high, low], axis=0
        )
        result_copy(i, z).start()
        return carry

    others = RING - 1 - z
    lax.fori_loop(0, jnp.minimum(others, 3), serve, 0)
    w.second_step(1, 0)
    lax.fori_loop(3, jnp.minimum(others, 5), serve, 0)
    w.second_step(1, 1)
    lax.fori_loop(5, others, serve, 0)
    w.second_step(2, 0)

    def combine(turn, carry):
        i = z - 1 - turn
        result_copy(i, i).wait_recv()
        spent = mine[:HEAD_DIM, :]
        low_at = HEAD_DIM + HEAD_DIM // 8
        more = returned[i, HEAD_DIM : HEAD_DIM + 1, :].astype(jnp.float32)
        more = more + returned[i, low_at : low_at + 1, :].astype(jnp.float32)
        mine[HEAD_DIM:, :] += jnp.exp2(-spent) * returned[i, :HEAD_DIM, :].astype(jnp.float32)
        mine[:HEAD_DIM, :] = spent + more
        return carry

    lax.fori_loop(0, z, combine, 0)
    sides = jnp.where(core == 0, 1.0, 0.0)
    found = mine[HEAD_DIM:, :]
    attended[...] = jnp.concatenate([found * sides, found * (1.0 - sides)], axis=0).T.astype(
        jnp.bfloat16
    )
    exchange = []
    for k in range(1, GROUP):
        peer = wrap(tp + k, GROUP)
        rows = pl.ds(pl.multiple_of(peer * own_rows, own_rows), own_rows)
        exchange.append(post.start(attended.at[rows], arrived.at[tp], {"tp": peer}))
    arrived[tp] = attended[pl.ds(pl.multiple_of(tp * own_rows, own_rows), own_rows), :]
    w.second_step(2, 1)
    for copy in loads[7:]:
        copy.wait()
    for copy in exchange:
        copy.wait_recv()
    heads = jnp.concatenate([arrived[2 * i] + arrived[2 * i + 1] for i in range(CHIPS)], axis=1)
    mixed = rounded(jnp.dot(heads, wout[...], preferred_element_type=jnp.float32))
    mid = rounded(resid[...].astype(jnp.float32) + gain_mix[...] * rms_scale(mixed))
    middle[...] = mid
    normed = rounded(gain_pre[...] * rms_scale(mid))

    right, left = wrap(x + 1, CHIPS), wrap(x - 1, CHIPS)

    def rows_of(chip, c, half=None):
        start = HALO + (2 * chip + c) * own_rows
        if half is None:
            return piece.at[pl.ds(pl.multiple_of(start, HALO), own_rows)]
        start = start + half * (own_rows // 2)
        return piece.at[pl.ds(pl.multiple_of(start, HALO), own_rows // 2)]

    def to_chip(chip):
        return {"tp": 2 * chip + core}

    partner = {"tp": 2 * x + 1 - core}

    def move(ref, device):
        return post.start(ref, ref, device)

    piece[pl.ds(pl.multiple_of(HALO + tp * own_rows, HALO), own_rows), :] = normed.astype(
        jnp.bfloat16
    )
    edge_out[...] = normed[own_rows - (KERNEL - 1) :, :]
    plus = [move(rows_of(x, core, 0), to_chip(right))]
    minus = [move(rows_of(x, core, 1), to_chip(left))]
    plus.append(move(rows_of(x, core, 1), to_chip(right)))
    minus.append(move(rows_of(x, core, 0), to_chip(left)))
    across = [move(rows_of(x, core), partner)]

    def edge_copy(src, device, slot):
        return pltpu.make_async_remote_copy(
            src_ref=src,
            dst_ref=edge_in,
            send_sem=edge_sem.at[slot],
            recv_sem=edge_sem.at[GROUP],
            device_id=device,
            device_id_type=MESH,
        )

    last = tp == GROUP - 1
    ahead = edge_copy(edge_out, {"sp": wrap(sp + 1, shards)}, 0)

    @pl.when(last & (sp < shards - 1))
    def _():
        ahead.start()

    plus[0].wait_recv()
    plus.append(move(rows_of(left, core, 0), to_chip(right)))
    across.append(move(rows_of(left, core, 0), partner))
    minus[0].wait_recv()
    minus.append(move(rows_of(right, core, 1), to_chip(left)))
    across.append(move(rows_of(right, core, 1), partner))
    plus[1].wait_recv()
    across.append(move(rows_of(left, core, 1), partner))
    minus[1].wait_recv()
    across.append(move(rows_of(right, core, 0), partner))
    far = wrap(x + 2, CHIPS)
    plus[2].wait_recv()
    across.append(move(rows_of(far, core, 0), partner))
    minus[2].wait_recv()
    across.append(move(rows_of(far, core, 1), partner))
    w.second_step(3, 0)

    spread = [edge_copy(edge_in, {"tp": wrap(tp + k, GROUP)}, k) for k in range(1, GROUP)]

    @pl.when(sp > 0)
    def _():
        spread[0].wait_recv()

        @pl.when(last)
        def _():
            for copy in spread:
                copy.start()

    behind = edge_in[...]
    place = lax.broadcasted_iota(jnp.int32, (HALO, piece.shape[1]), 0)
    front = jnp.where(sp > 0, 1, 0)
    filled = jnp.where(
        (place == HALO - 1) & (front == 1),
        behind[1:2, :],
        jnp.where((place == HALO - 2) & (front == 1), behind[0:1, :], 0.0),
    )
    piece[0:HALO, :] = filled.astype(jnp.bfloat16)
    for copy in across:
        copy.wait_recv()
    w.second_step(3, 1)
    w.second_step(4, 0)
    w.second_step(4, 1)

    depth = piece.shape[1]

    def convolve(low, high, taps):
        rows = partial.shape[0] * own_rows
        found = 0.0
        for tap in range(KERNEL):
            found = found + taps[tap : tap + 1, :] * extended[
                pl.ds(HALO - KERNEL + 1 + tap, rows), low:high
            ]
        return found

    def silu(v):
        return v / (1.0 + jnp.exp(-v))

    for j in range(mains):
        cols = slice(2 * j * LANES, (2 * j + 2) * LANES)
        rhs = whole[:, :, :, cols].reshape(depth, 2 * LANES)
        extended[...] = rounded(jnp.dot(piece[...], rhs, preferred_element_type=jnp.float32))
        here = slice(j * LANES, (j + 1) * LANES)
        g = convolve(0, LANES, conv_gate[:, here])
        u = convolve(LANES, 2 * LANES, conv_up[:, here])
        hidden[:, here] = (silu(g) * u).astype(jnp.bfloat16)
    rhs = whole[:, :, :, base : base + LANES].reshape(depth, LANES)
    extended[:, :LANES] = rounded(jnp.dot(piece[...], rhs, preferred_element_type=jnp.float32))
    taps = jnp.concatenate([conv_gate[:, mains * LANES :], conv_up[:, mains * LANES :]], axis=1)
    both = convolve(0, LANES, taps)
    product = silu(both) * pltpu.roll(both, LANES - rest, axis=1)
    inside = lax.broadcasted_iota(jnp.int32, product.shape, 1) < rest
    hidden[:, mains * LANES :] = jnp.where(inside, product, 0.0).astype(jnp.bfloat16)

    for j in range(RING):
        rhs = whole[j, :, :, down_at:].reshape(depth // RING, hidden.shape[1])
        found = lax.dot_general(
            hidden[...], rhs, (((1,), (1,)), ((), ())), preferred_element_type=jnp.float32
        )
        partial[:, :, j * (depth // RING) : (j + 1) * (depth // RING)] = found.astype(
            jnp.bfloat16
        ).reshape(partial.shape[0], own_rows, depth // RING)

    swaps = [
        post.start(partial.at[2 * chip + 1 - core], partner_partial.at[chip], partner)
        for chip in range(CHIPS)
    ]
    halves = (pl.ds(0, own_rows // 2), pl.ds(own_rows // 2, own_rows // 2))
    for copy in swaps:
        copy.wait_recv()
    for chip in range(CHIPS):
        summed[chip] = (
            partial[2 * chip + core].astype(jnp.float32)
            + partner_partial[chip].astype(jnp.float32)
        ).astype(jnp.bfloat16)

    def give(src, slot, chip):
        return post.start(src, landed.at[slot], to_chip(chip))

    got = [
        give(summed.at[far, halves[0]], 0, right),
        give(summed.at[far, halves[1]], 1, left),
        give(summed.at[right, halves[1]], 2, right),
        give(summed.at[left, halves[0]], 3, left),
    ]
    got[0].wait_recv()
    passed[0] = (
        summed[right, halves[0], :].astype(jnp.float32) + landed[0].astype(jnp.float32)
    ).astype(jnp.bfloat16)
    got.append(give(passed.at[0], 4, right))
    got[1].wait_recv()
    passed[1] = (
        summed[left, halves[1], :].astype(jnp.float32) + landed[1].astype(jnp.float32)
    ).astype(jnp.bfloat16)
    got.append(give(passed.at[1], 5, left))
    for copy in got[2:]:
        copy.wait_recv()
    for h, (near, through) in enumerate(((3, 4), (2, 5))):
        ffn = rounded(
            summed[x, halves[h], :].astype(jnp.float32)
            + landed[near].astype(jnp.float32)
            + landed[through].astype(jnp.float32)
        )
        result[halves[h], :] = (
            middle[halves[h], :] + gain_post[...] * rms_scale(ffn)
        ).astype(jnp.bfloat16)

    post.drain()

    def sent(turn, carry):
        result_copy(z + 1 + turn, z).wait_send()
        return carry

    lax.fori_loop(0, others, sent, 0)

    @pl.when(last & (sp < shards - 1))
    def _():
        ahead.wait_send()

    @pl.when(last & (sp > 0))
    def _():
        for copy in spread:
            copy.wait_send()


def local(
    queries,
    keys,
    values,
    score_shift,
    resid,
    w_out,
    gain_mix,
    gain_pre,
    w_gate,
    w_up,
    conv_gate,
    conv_up,
    w_down,
    gain_post,
):
    span = queries.shape[0]
    own_rows, depth = resid.shape
    width = w_gate.shape[1]
    mains = width // LANES
    slab = w_gate.shape[0]
    columns = 2 * mains * LANES + LANES + (mains + 1) * LANES
    vmem = pl.BlockSpec(memory_space=pltpu.VMEM)
    hbm = pl.BlockSpec(memory_space=pltpu.HBM)
    bf16, f32 = jnp.bfloat16, jnp.float32
    return pl.pallas_call(
        layer_kernel,
        out_shape=jax.ShapeDtypeStruct((own_rows, depth), bf16),
        in_specs=[hbm] * 14,
        out_specs=vmem,
        scratch_shapes=[
            pltpu.SMEM((1,), f32),
            pltpu.VMEM((1, depth), f32),
            pltpu.VMEM((1, depth), f32),
            pltpu.VMEM((1, depth), f32),
            pltpu.VMEM(conv_gate.shape, f32),
            pltpu.VMEM(conv_up.shape, f32),
            pltpu.VMEM((RING, HEAD_DIM, span), bf16),
            pltpu.VMEM((span, LANES), bf16),
            pltpu.VMEM((RING, 2 * HEAD_DIM, span), bf16),
            pltpu.VMEM((slab, width), bf16),
            pltpu.VMEM((slab, width), bf16),
            pltpu.VMEM((slab, width), bf16),
            pltpu.VMEM((RING, RING, slab, columns), bf16),
            pltpu.VMEM((own_rows, depth), bf16),
            pltpu.VMEM(w_out.shape, bf16),
            pltpu.VMEM((span, span), bf16),
            pltpu.VMEM((span, LANES), f32),
            pltpu.VMEM((span, LANES), f32),
            pltpu.VMEM((span, LANES), bf16),
            pltpu.VMEM((RING, HEAD_DIM + HEAD_DIM // 4, span), bf16),
            pltpu.VMEM((RING, HEAD_DIM + HEAD_DIM // 4, span), bf16),
            pltpu.VMEM((2 * HEAD_DIM, span), f32),
            pltpu.VMEM((GROUP, own_rows, LANES), bf16),
            pltpu.VMEM((HALO + span, depth), bf16),
            pltpu.VMEM((own_rows, depth), f32),
            pltpu.VMEM((KERNEL - 1, depth), f32),
            pltpu.VMEM((KERNEL - 1, depth), f32),
            pltpu.VMEM((HALO + span, 2 * LANES), f32),
            pltpu.VMEM((span, (mains + 1) * LANES), bf16),
            pltpu.VMEM((GROUP, own_rows, depth), bf16),
            pltpu.VMEM((CHIPS, own_rows, depth), bf16),
            pltpu.VMEM((CHIPS, own_rows, depth), bf16),
            pltpu.VMEM((6, own_rows // 2, depth), bf16),
            pltpu.VMEM((2, own_rows // 2, depth), bf16),
            pltpu.SemaphoreType.DMA((TRANSFERS,)),
            pltpu.SemaphoreType.DMA((TRANSFERS,)),
            pltpu.SemaphoreType.DMA((LOADS,)),
            pltpu.SemaphoreType.DMA((GROUP + 1,)),
            pltpu.SemaphoreType.DMA((RING,)),
            pltpu.SemaphoreType.DMA((RING,)),
        ],
        compiler_params=pltpu.CompilerParams(
            collective_id=0, has_side_effects=True, vmem_limit_bytes=67_043_328
        ),
        name="layer",
    )(
        score_shift,
        gain_mix[None],
        gain_pre[None],
        gain_post[None],
        conv_gate,
        conv_up,
        queries.T,
        keys.T,
        values.T,
        w_gate,
        w_up,
        w_down.T,
        resid,
        w_out,
    )


def solution(mesh):
    in_specs = (
        P("sp", "tp"),
        P("sp", "tp"),
        P("sp", "tp"),
        P("tp"),
        P(("sp", "tp"), None),
        P(),
        P(),
        P(),
        P("sp", "tp"),
        P("sp", "tp"),
        P(None, "tp"),
        P(None, "tp"),
        P("tp", "sp"),
        P(),
    )
    out_specs = P(("sp", "tp"), None)
    return jax.shard_map(local, mesh=mesh, in_specs=in_specs, out_specs=out_specs, check_vma=False)
```

```python
import math

import jax
import jax.numpy as jnp
from jax import lax
from jax.experimental import pallas as pl
from jax.experimental.pallas import tpu as pltpu
from jax.sharding import PartitionSpec as P

HEAD_DIM = 64
KERNEL = 3
RING = 8
CHIPS = 4
GROUP = 8
MESH = pl.DeviceIdType.MESH
LOG2E = 1.0 / math.log(2.0)
LANES = 128
HALO = 16
UNROLL = 4
TRANSFERS = 256
LOADS = 14


def wrap(v, n):
    return lax.rem(v + 2 * n, n)


class Post:
    def __init__(self, send, recv):
        self.send, self.recv, self.copies = send, recv, []

    def start(self, src, dst, device):
        slot = len(self.copies)
        copy = pltpu.make_async_remote_copy(
            src_ref=src,
            dst_ref=dst,
            send_sem=self.send.at[slot],
            recv_sem=self.recv.at[slot],
            device_id=device,
            device_id_type=MESH,
        )
        copy.start()
        self.copies.append(copy)
        return copy

    def drain(self):
        for copy in self.copies:
            copy.wait_send()


class Line:
    def __init__(self, post, me, place, device):
        self.post, self.me, self.place, self.device = post, me, place, device
        self.copies = {}

    def step(self, s):
        for sign in (1, -1):
            if (sign, s - 1) in self.copies:
                self.copies[(sign, s - 1)].wait_recv()
            if s < RING // 2:
                part = None if s < RING // 2 - 1 else (0 if sign == 1 else 1)
                ref = self.place(wrap(self.me - sign * s, RING), part)
                self.copies[(sign, s)] = self.post.start(
                    ref, ref, self.device(wrap(self.me + sign, RING))
                )


class Rings:
    ORDER = (0, -1, 1, -2, 2, -3, 3, -4)

    def __init__(self, post, z, y, buf):
        self.post, self.z, self.y, self.buf = post, z, y, buf
        tiles = buf.shape[3] // LANES
        split = tiles // 2 * LANES
        self.part = (pl.ds(0, split), pl.ds(split, buf.shape[3] - split))
        self.copies = {}

    def _neighbour(self, along_y, sign):
        if along_y:
            return {"sp": self.z * RING + wrap(self.y + sign, RING)}
        return {"sp": wrap(self.z + sign, RING) * RING + self.y}

    def _place(self, h, first, second):
        if h == 0:
            z, y = wrap(self.z + second, RING), wrap(self.y + first, RING)
        else:
            z, y = wrap(self.z + first, RING), wrap(self.y + second, RING)
        return self.buf.at[z, y, :, self.part[h]]

    def _carries(self, h, sign, at):
        return sign == -1 if h == 0 else (at < RING // 2) == (sign == 1)

    def first_step(self, s):
        for h in (0, 1):
            for sign in (1, -1):
                if (1, h, sign, s - 1) in self.copies:
                    self.copies[(1, h, sign, s - 1)].wait_recv()
                if s < (4 if sign == 1 else 3):
                    place = self._place(h, -sign * s, 0)
                    self.copies[(1, h, sign, s)] = self.post.start(
                        place, place, self._neighbour(h == 0, sign)
                    )

    def second_step(self, s, low, high):
        for at in range(low, high):
            for h in (0, 1):
                for sign in (1, -1):
                    if (2, h, sign, s - 1, at) in self.copies:
                        self.copies[(2, h, sign, s - 1, at)].wait_recv()
                    if s < 3 or (s == 3 and self._carries(h, sign, at)):
                        place = self._place(h, self.ORDER[at], -sign * s)
                        self.copies[(2, h, sign, s, at)] = self.post.start(
                            place, place, self._neighbour(h == 1, sign)
                        )


def tile(query, pair, tri, shift2, own):
    raw = jnp.dot(query, pair, preferred_element_type=jnp.float32)
    t = raw * (LOG2E * HEAD_DIM**-0.5) - shift2
    spent = jnp.maximum(t, jnp.log(1.0 + jnp.exp2(jnp.minimum(t, 126.0))) * LOG2E)
    taken = t - spent
    if own:
        row = lax.broadcasted_iota(jnp.int32, t.shape, 0)
        col = lax.broadcasted_iota(jnp.int32, t.shape, 1)
        causal = col < row
        spent = jnp.where(causal, spent, 0.0)
    later = jnp.dot(spent.astype(jnp.bfloat16), tri, preferred_element_type=jnp.float32)
    weights = jnp.exp2(taken - later)
    if own:
        weights = jnp.where(causal, weights, 0.0)
    total = jnp.broadcast_to(later[:, :1] + spent[:, :1], (t.shape[0], LANES))
    out = lax.dot_general(
        weights.astype(jnp.bfloat16),
        pair,
        (((1,), (1,)), ((), ())),
        preferred_element_type=jnp.float32,
    )
    return out, total


def rms_scale(v):
    return v * lax.rsqrt(jnp.mean(v * v, axis=-1, keepdims=True) + 1e-06)


def rounded(v):
    return v.astype(jnp.bfloat16).astype(jnp.float32)


def layer_kernel(
    shift_hbm,
    mix_hbm,
    pre_hbm,
    post_hbm,
    conv_gate_hbm,
    conv_up_hbm,
    q_hbm,
    k_hbm,
    v_hbm,
    gate_hbm,
    up_hbm,
    down_hbm,
    resid_hbm,
    wout_hbm,
    result,
    shift_ref,
    gain_mix,
    gain_pre,
    gain_post,
    conv_gate,
    conv_up,
    queries,
    query,
    pairs,
    gate,
    up,
    down,
    whole,
    resid,
    wout,
    tri,
    acc,
    tail,
    attended,
    messages,
    returned,
    mine,
    arrived,
    piece,
    middle,
    edge_out,
    edge_in,
    extended,
    hidden,
    partial,
    partner_partial,
    summed,
    landed,
    passed,
    send,
    recv,
    load,
    edge_sem,
    give_sem,
    take_sem,
):
    sp, tp = lax.axis_index("sp"), lax.axis_index("tp")
    z, y = lax.div(sp, RING), lax.rem(sp, RING)
    x, core = lax.div(tp, 2), lax.rem(tp, 2)
    shards = RING * RING
    span = query.shape[0]
    own_rows = result.shape[0]
    width = gate.shape[1]
    mains = width // LANES
    rest = width - mains * LANES

    loads = [
        pltpu.make_async_copy(a, b, load.at[i])
        for i, (a, b) in enumerate(
            (
                (k_hbm, pairs.at[y, pl.ds(0, HEAD_DIM)]),
                (v_hbm, pairs.at[y, pl.ds(HEAD_DIM, HEAD_DIM)]),
                (q_hbm, queries.at[z]),
                (gate_hbm, gate),
                (up_hbm, up),
                (down_hbm, down),
                (shift_hbm, shift_ref),
                (resid_hbm, resid),
                (wout_hbm, wout),
                (mix_hbm, gain_mix),
                (pre_hbm, gain_pre),
                (post_hbm, gain_post),
                (conv_gate_hbm, conv_gate),
                (conv_up_hbm, conv_up),
            )
        )
    ]
    for copy in loads:
        copy.start()
    barrier = pltpu.get_barrier_semaphore()
    greeted = [{"sp": z * RING + wrap(y + k, RING)} for k in (1, -1)]
    greeted += [{"sp": wrap(z + k, RING) * RING + y} for k in range(1, RING)]
    greeted += [{"sp": wrap(sp + 1, shards)}, {"sp": wrap(sp - 1, shards)}]
    greeted += [{"tp": wrap(tp + k, GROUP)} for k in range(1, GROUP)]
    for device in greeted:
        pl.semaphore_signal(barrier, inc=1, device_id=device, device_id_type=MESH)
    for copy in loads[3:6]:
        copy.wait()
    for j in range(mains):
        here = slice(j * LANES, (j + 1) * LANES)
        whole[z, y, :, 2 * j * LANES : (2 * j + 1) * LANES] = gate[:, here]
        whole[z, y, :, (2 * j + 1) * LANES : (2 * j + 2) * LANES] = up[:, here]
    base = 2 * mains * LANES
    whole[z, y, :, base : base + LANES] = jnp.concatenate(
        [gate[:, mains * LANES :], up[:, mains * LANES :]], axis=1
    )
    down_at = base + LANES
    whole[z, y, :, down_at : down_at + mains * LANES] = down[:, : mains * LANES]
    whole[z, y, :, down_at + mains * LANES :] = jnp.concatenate(
        [down[:, mains * LANES :], jnp.zeros((down.shape[0], LANES - rest), jnp.bfloat16)], axis=1
    )
    for copy in loads[:3]:
        copy.wait()
    pl.semaphore_wait(barrier, len(greeted))

    post = Post(send, recv)

    def key_place(i, part):
        return pairs.at[i] if part is None else pairs.at[i, pl.ds(part * HEAD_DIM, HEAD_DIM)]

    def query_place(i, part):
        half = HEAD_DIM // 2
        return queries.at[i] if part is None else queries.at[i, pl.ds(part * half, half)]

    kv = Line(post, y, key_place, lambda i: {"sp": z * RING + i})
    qs = Line(post, z, query_place, lambda i: {"sp": i * RING + y})
    w = Rings(post, z, y, whole)
    kv.step(0)
    qs.step(0)
    w.first_step(0)
    w.second_step(0, 0, 1)

    at = lax.broadcasted_iota(jnp.int32, tri.shape, 0)
    to = lax.broadcasted_iota(jnp.int32, tri.shape, 1)
    tri[...] = jnp.where(at > to, 1.0, 0.0).astype(jnp.bfloat16)
    loads[6].wait()
    shift2 = shift_ref[0] * LOG2E

    def set_query(i):
        padded = jnp.concatenate(
            [queries[i].astype(jnp.float32), jnp.zeros(queries.shape[1:], jnp.float32)], axis=0
        )
        query[...] = padded.T.astype(jnp.bfloat16)

    def visit(first, count, fresh=False):
        found = [
            tile(query[...], pairs[first - k], tri[...], shift2, False) for k in range(count)
        ]
        if fresh:
            total, spent = found.pop(0)
        else:
            total, spent = acc[...], tail[...]
        for out, more in found:
            total = total + jnp.exp2(-spent) * out
            spent = spent + more
        acc[...] = total
        tail[...] = spent

    def report():
        lane = lax.broadcasted_iota(jnp.int32, acc.shape, 1)
        return jnp.where(lane < HEAD_DIM, tail[...], acc[...]).T

    kv.step(1)
    qs.step(1)
    w.first_step(1)
    w.second_step(0, 1, 2)
    set_query(z)
    first_out, first_tail = tile(query[...], pairs[y], tri[...], shift2, True)
    acc[...] = first_out
    tail[...] = first_tail
    for s in (2, 3):
        kv.step(s)
        qs.step(s)
        w.first_step(s)
        w.second_step(0, s, s + 1)
    kv.step(4)
    qs.step(4)
    w.first_step(4)
    w.second_step(0, 4, 8)

    def one(turn, carry):
        visit(y - 1 - turn, 1)
        return carry

    def several(turn, carry):
        visit(y - 1 - lax.rem(y, UNROLL) - turn * UNROLL, UNROLL)
        return carry

    lax.fori_loop(0, lax.rem(y, UNROLL), one, 0)
    lax.fori_loop(0, lax.div(y, UNROLL), several, 0)
    mine[...] = report()

    def result_copy(i, there):
        return pltpu.make_async_remote_copy(
            src_ref=messages.at[i],
            dst_ref=returned.at[there],
            send_sem=give_sem.at[i],
            recv_sem=take_sem.at[there],
            device_id={"sp": i * RING + y},
            device_id_type=MESH,
        )

    def serve(turn, carry):
        i = z + 1 + turn
        set_query(i)
        visit(RING - 1, UNROLL, fresh=True)
        visit(RING - 1 - UNROLL, UNROLL)
        found = report()
        spent = found[: HEAD_DIM // 8, :]
        high = spent.astype(jnp.bfloat16)
        low = (spent - high.astype(jnp.float32)).astype(jnp.bfloat16)
        messages[i] = jnp.concatenate(
            [found[HEAD_DIM:, :].astype(jnp.bfloat16), high, low], axis=0
        )
        result_copy(i, z).start()
        return carry

    others = RING - 1 - z
    lax.fori_loop(0, jnp.minimum(others, 1), serve, 0)
    w.second_step(1, 0, 4)
    lax.fori_loop(1, jnp.minimum(others, 4), serve, 0)
    w.second_step(1, 4, 8)
    lax.fori_loop(4, others, serve, 0)
    w.second_step(2, 0, 4)

    def combine(turn, carry):
        i = z - 1 - turn
        result_copy(i, i).wait_recv()
        spent = mine[:HEAD_DIM, :]
        low_at = HEAD_DIM + HEAD_DIM // 8
        more = returned[i, HEAD_DIM : HEAD_DIM + 1, :].astype(jnp.float32)
        more = more + returned[i, low_at : low_at + 1, :].astype(jnp.float32)
        mine[HEAD_DIM:, :] += jnp.exp2(-spent) * returned[i, :HEAD_DIM, :].astype(jnp.float32)
        mine[:HEAD_DIM, :] = spent + more
        return carry

    lax.fori_loop(0, z, combine, 0)
    sides = jnp.where(core == 0, 1.0, 0.0)
    found = mine[HEAD_DIM:, :]
    attended[...] = jnp.concatenate([found * sides, found * (1.0 - sides)], axis=0).T.astype(
        jnp.bfloat16
    )
    exchange = []
    for k in range(1, GROUP):
        peer = wrap(tp + k, GROUP)
        rows = pl.ds(pl.multiple_of(peer * own_rows, own_rows), own_rows)
        exchange.append(post.start(attended.at[rows], arrived.at[tp], {"tp": peer}))
    arrived[tp] = attended[pl.ds(pl.multiple_of(tp * own_rows, own_rows), own_rows), :]
    w.second_step(2, 4, 8)
    for copy in loads[7:]:
        copy.wait()
    for copy in exchange:
        copy.wait_recv()
    heads = jnp.concatenate([arrived[2 * i] + arrived[2 * i + 1] for i in range(CHIPS)], axis=1)
    mixed = rounded(jnp.dot(heads, wout[...], preferred_element_type=jnp.float32))
    mid = rounded(resid[...].astype(jnp.float32) + gain_mix[...] * rms_scale(mixed))
    middle[...] = mid
    normed = rounded(gain_pre[...] * rms_scale(mid))

    right, left = wrap(x + 1, CHIPS), wrap(x - 1, CHIPS)

    def rows_of(chip, c, half=None):
        start = HALO + (2 * chip + c) * own_rows
        if half is None:
            return piece.at[pl.ds(pl.multiple_of(start, HALO), own_rows)]
        start = start + half * (own_rows // 2)
        return piece.at[pl.ds(pl.multiple_of(start, HALO), own_rows // 2)]

    def to_chip(chip):
        return {"tp": 2 * chip + core}

    partner = {"tp": 2 * x + 1 - core}

    def move(ref, device):
        return post.start(ref, ref, device)

    piece[pl.ds(pl.multiple_of(HALO + tp * own_rows, HALO), own_rows), :] = normed.astype(
        jnp.bfloat16
    )
    edge_out[...] = normed[own_rows - (KERNEL - 1) :, :]
    plus = [move(rows_of(x, core, 0), to_chip(right))]
    minus = [move(rows_of(x, core, 1), to_chip(left))]
    plus.append(move(rows_of(x, core, 1), to_chip(right)))
    minus.append(move(rows_of(x, core, 0), to_chip(left)))
    across = [move(rows_of(x, core), partner)]

    def edge_copy(src, device, slot):
        return pltpu.make_async_remote_copy(
            src_ref=src,
            dst_ref=edge_in,
            send_sem=edge_sem.at[slot],
            recv_sem=edge_sem.at[GROUP],
            device_id=device,
            device_id_type=MESH,
        )

    last = tp == GROUP - 1
    ahead = edge_copy(edge_out, {"sp": wrap(sp + 1, shards)}, 0)

    @pl.when(last & (sp < shards - 1))
    def _():
        ahead.start()

    w.second_step(3, 0, 4)
    plus[0].wait_recv()
    plus.append(move(rows_of(left, core, 0), to_chip(right)))
    across.append(move(rows_of(left, core, 0), partner))
    minus[0].wait_recv()
    minus.append(move(rows_of(right, core, 1), to_chip(left)))
    across.append(move(rows_of(right, core, 1), partner))
    plus[1].wait_recv()
    across.append(move(rows_of(left, core, 1), partner))
    minus[1].wait_recv()
    across.append(move(rows_of(right, core, 0), partner))
    far = wrap(x + 2, CHIPS)
    plus[2].wait_recv()
    across.append(move(rows_of(far, core, 0), partner))
    minus[2].wait_recv()
    across.append(move(rows_of(far, core, 1), partner))

    spread = [edge_copy(edge_in, {"tp": wrap(tp + k, GROUP)}, k) for k in range(1, GROUP)]

    @pl.when(sp > 0)
    def _():
        spread[0].wait_recv()

        @pl.when(last)
        def _():
            for copy in spread:
                copy.start()

    behind = edge_in[...]
    place = lax.broadcasted_iota(jnp.int32, (HALO, piece.shape[1]), 0)
    front = jnp.where(sp > 0, 1, 0)
    filled = jnp.where(
        (place == HALO - 1) & (front == 1),
        behind[1:2, :],
        jnp.where((place == HALO - 2) & (front == 1), behind[0:1, :], 0.0),
    )
    piece[0:HALO, :] = filled.astype(jnp.bfloat16)
    for copy in across:
        copy.wait_recv()
    w.second_step(3, 4, 8)
    w.second_step(4, 0, 4)
    w.second_step(4, 4, 8)

    depth = piece.shape[1]

    def convolve(low, high, taps):
        rows = partial.shape[0] * own_rows
        found = 0.0
        for tap in range(KERNEL):
            found = found + taps[tap : tap + 1, :] * extended[
                pl.ds(HALO - KERNEL + 1 + tap, rows), low:high
            ]
        return found

    def silu(v):
        return v / (1.0 + jnp.exp(-v))

    for j in range(mains):
        cols = slice(2 * j * LANES, (2 * j + 2) * LANES)
        rhs = whole[:, :, :, cols].reshape(depth, 2 * LANES)
        extended[...] = rounded(jnp.dot(piece[...], rhs, preferred_element_type=jnp.float32))
        here = slice(j * LANES, (j + 1) * LANES)
        g = convolve(0, LANES, conv_gate[:, here])
        u = convolve(LANES, 2 * LANES, conv_up[:, here])
        hidden[:, here] = (silu(g) * u).astype(jnp.bfloat16)
    rhs = whole[:, :, :, base : base + LANES].reshape(depth, LANES)
    extended[:, :LANES] = rounded(jnp.dot(piece[...], rhs, preferred_element_type=jnp.float32))
    taps = jnp.concatenate([conv_gate[:, mains * LANES :], conv_up[:, mains * LANES :]], axis=1)
    both = convolve(0, LANES, taps)
    product = silu(both) * pltpu.roll(both, LANES - rest, axis=1)
    inside = lax.broadcasted_iota(jnp.int32, product.shape, 1) < rest
    hidden[:, mains * LANES :] = jnp.where(inside, product, 0.0).astype(jnp.bfloat16)

    stripe = depth // RING
    wide = depth // 2
    sides_of = [pl.ds(0, wide), pl.ds(wide, wide)]
    halves = (pl.ds(0, own_rows // 2), pl.ds(own_rows // 2, own_rows // 2))
    swaps = []
    for part in (0, 1):
        for j in range(part * RING // 2, (part + 1) * RING // 2):
            rhs = whole[j, :, :, down_at:].reshape(stripe, hidden.shape[1])
            found = lax.dot_general(
                hidden[...], rhs, (((1,), (1,)), ((), ())), preferred_element_type=jnp.float32
            )
            partial[:, :, j * stripe : (j + 1) * stripe] = found.astype(jnp.bfloat16).reshape(
                partial.shape[0], own_rows, stripe
            )
        swaps.append(
            [
                post.start(
                    partial.at[2 * chip + 1 - core, :, sides_of[part]],
                    partner_partial.at[chip, :, sides_of[part]],
                    partner,
                )
                for chip in (far, right, left, x)
            ]
        )

    def give(src, slot, part, chip):
        return post.start(src, landed.at[slot, :, sides_of[part]], to_chip(chip))

    got = []
    for part in (0, 1):
        cols = sides_of[part]
        for copy in swaps[part]:
            copy.wait_recv()
        for chip in (far, right, left, x):
            summed[chip, :, cols] = (
                partial[2 * chip + core, :, cols].astype(jnp.float32)
                + partner_partial[chip, :, cols].astype(jnp.float32)
            ).astype(jnp.bfloat16)
        got.append(
            [
                give(summed.at[far, halves[0], cols], 0, part, right),
                give(summed.at[far, halves[1], cols], 1, part, left),
                give(summed.at[right, halves[1], cols], 2, part, right),
                give(summed.at[left, halves[0], cols], 3, part, left),
            ]
        )
    for part in (0, 1):
        cols = sides_of[part]
        for k, (toward, half) in enumerate(((right, 0), (left, 1))):
            got[part][k].wait_recv()
            passed[k, :, cols] = (
                summed[toward, halves[half], cols].astype(jnp.float32)
                + landed[k, :, cols].astype(jnp.float32)
            ).astype(jnp.bfloat16)
            got[part].append(give(passed.at[k, :, cols], 4 + k, part, toward))
    for part in (0, 1):
        for copy in got[part][2:]:
            copy.wait_recv()
    for h, (near, through) in enumerate(((3, 4), (2, 5))):
        ffn = rounded(
            summed[x, halves[h], :].astype(jnp.float32)
            + landed[near].astype(jnp.float32)
            + landed[through].astype(jnp.float32)
        )
        result[halves[h], :] = (
            middle[halves[h], :] + gain_post[...] * rms_scale(ffn)
        ).astype(jnp.bfloat16)

    post.drain()

    def sent(turn, carry):
        result_copy(z + 1 + turn, z).wait_send()
        return carry

    lax.fori_loop(0, others, sent, 0)

    @pl.when(last & (sp < shards - 1))
    def _():
        ahead.wait_send()

    @pl.when(last & (sp > 0))
    def _():
        for copy in spread:
            copy.wait_send()


def local(
    queries,
    keys,
    values,
    score_shift,
    resid,
    w_out,
    gain_mix,
    gain_pre,
    w_gate,
    w_up,
    conv_gate,
    conv_up,
    w_down,
    gain_post,
):
    span = queries.shape[0]
    own_rows, depth = resid.shape
    width = w_gate.shape[1]
    mains = width // LANES
    slab = w_gate.shape[0]
    columns = 2 * mains * LANES + LANES + (mains + 1) * LANES
    vmem = pl.BlockSpec(memory_space=pltpu.VMEM)
    hbm = pl.BlockSpec(memory_space=pltpu.HBM)
    bf16, f32 = jnp.bfloat16, jnp.float32
    return pl.pallas_call(
        layer_kernel,
        out_shape=jax.ShapeDtypeStruct((own_rows, depth), bf16),
        in_specs=[hbm] * 14,
        out_specs=vmem,
        scratch_shapes=[
            pltpu.SMEM((1,), f32),
            pltpu.VMEM((1, depth), f32),
            pltpu.VMEM((1, depth), f32),
            pltpu.VMEM((1, depth), f32),
            pltpu.VMEM(conv_gate.shape, f32),
            pltpu.VMEM(conv_up.shape, f32),
            pltpu.VMEM((RING, HEAD_DIM, span), bf16),
            pltpu.VMEM((span, LANES), bf16),
            pltpu.VMEM((RING, 2 * HEAD_DIM, span), bf16),
            pltpu.VMEM((slab, width), bf16),
            pltpu.VMEM((slab, width), bf16),
            pltpu.VMEM((slab, width), bf16),
            pltpu.VMEM((RING, RING, slab, columns), bf16),
            pltpu.VMEM((own_rows, depth), bf16),
            pltpu.VMEM(w_out.shape, bf16),
            pltpu.VMEM((span, span), bf16),
            pltpu.VMEM((span, LANES), f32),
            pltpu.VMEM((span, LANES), f32),
            pltpu.VMEM((span, LANES), bf16),
            pltpu.VMEM((RING, HEAD_DIM + HEAD_DIM // 4, span), bf16),
            pltpu.VMEM((RING, HEAD_DIM + HEAD_DIM // 4, span), bf16),
            pltpu.VMEM((2 * HEAD_DIM, span), f32),
            pltpu.VMEM((GROUP, own_rows, LANES), bf16),
            pltpu.VMEM((HALO + span, depth), bf16),
            pltpu.VMEM((own_rows, depth), f32),
            pltpu.VMEM((KERNEL - 1, depth), f32),
            pltpu.VMEM((KERNEL - 1, depth), f32),
            pltpu.VMEM((HALO + span, 2 * LANES), f32),
            pltpu.VMEM((span, (mains + 1) * LANES), bf16),
            pltpu.VMEM((GROUP, own_rows, depth), bf16),
            pltpu.VMEM((CHIPS, own_rows, depth), bf16),
            pltpu.VMEM((CHIPS, own_rows, depth), bf16),
            pltpu.VMEM((6, own_rows // 2, depth), bf16),
            pltpu.VMEM((2, own_rows // 2, depth), bf16),
            pltpu.SemaphoreType.DMA((TRANSFERS,)),
            pltpu.SemaphoreType.DMA((TRANSFERS,)),
            pltpu.SemaphoreType.DMA((LOADS,)),
            pltpu.SemaphoreType.DMA((GROUP + 1,)),
            pltpu.SemaphoreType.DMA((RING,)),
            pltpu.SemaphoreType.DMA((RING,)),
        ],
        compiler_params=pltpu.CompilerParams(
            collective_id=0, has_side_effects=True, vmem_limit_bytes=67_043_328
        ),
        name="layer",
    )(
        score_shift,
        gain_mix[None],
        gain_pre[None],
        gain_post[None],
        conv_gate,
        conv_up,
        queries.T,
        keys.T,
        values.T,
        w_gate,
        w_up,
        w_down.T,
        resid,
        w_out,
    )


def solution(mesh):
    in_specs = (
        P("sp", "tp"),
        P("sp", "tp"),
        P("sp", "tp"),
        P("tp"),
        P(("sp", "tp"), None),
        P(),
        P(),
        P(),
        P("sp", "tp"),
        P("sp", "tp"),
        P(None, "tp"),
        P(None, "tp"),
        P("tp", "sp"),
        P(),
    )
    out_specs = P(("sp", "tp"), None)
    return jax.shard_map(local, mesh=mesh, in_specs=in_specs, out_specs=out_specs, check_vma=False)
```

```python
import math

import jax
import jax.numpy as jnp
from jax import lax
from jax.experimental import pallas as pl
from jax.experimental.pallas import tpu as pltpu
from jax.sharding import PartitionSpec as P

HEAD_DIM = 64
KERNEL = 3
RING = 8
CHIPS = 4
GROUP = 8
MESH = pl.DeviceIdType.MESH
LOG2E = 1.0 / math.log(2.0)
LANES = 128
HALO = 16
UNROLL = 4
KINDS = 10
ARRIVALS = 52
LOADS = 14


def wrap(v, n):
    return lax.rem(v + 2 * n, n)


class Post:
    def __init__(self, send, recv):
        self.send, self.recv = send, recv
        self.kinds, self.slots = 0, 0

    def kind(self):
        self.kinds += 1
        return self.send.at[self.kinds - 1]

    def slot(self):
        self.slots += 1
        return self.recv.at[self.slots - 1]


def remote(src, dst, sent, got, device):
    return pltpu.make_async_remote_copy(
        src_ref=src,
        dst_ref=dst,
        send_sem=sent,
        recv_sem=got,
        device_id=device,
        device_id_type=MESH,
    )


def started(*arguments):
    copy = remote(*arguments)
    copy.start()
    return copy


class Line:
    def __init__(self, post, me, place, device):
        self.post, self.me, self.place, self.device = post, me, place, device
        self.sent, self.copies = post.kind(), {}

    def step(self, s):
        for sign in (1, -1):
            if (sign, s - 1) in self.copies:
                self.copies[(sign, s - 1)].wait_recv()
            if s < RING // 2:
                part = None if s < RING // 2 - 1 else (0 if sign == 1 else 1)
                ref = self.place(wrap(self.me - sign * s, RING), part)
                device = self.device(wrap(self.me + sign, RING))
                self.copies[(sign, s)] = started(ref, ref, self.sent, self.post.slot(), device)

    def drain(self, whole):
        device = self.device(wrap(self.me + 1, RING))
        remote(whole, whole, self.sent, self.sent, device).wait_send()


class Rings:
    STEPS = RING // 2

    def __init__(self, post, z, y, buf, recv):
        self.post, self.z, self.y, self.buf, self.recv = post, z, y, buf, recv
        self.sent = [[post.kind() for _ in range(2)] for _ in range(2)]
        tiles = buf.shape[3] // LANES
        split = tiles // 2 * LANES
        self.part = (pl.ds(0, split), pl.ds(split, buf.shape[3] - split))
        self.copies = {}

    def _neighbour(self, along_y, sign):
        if along_y:
            return {"sp": self.z * RING + wrap(self.y + sign, RING)}
        return {"sp": wrap(self.z + sign, RING) * RING + self.y}

    def _place(self, h, first, second):
        if h == 0:
            z, y = wrap(self.z + second, RING), wrap(self.y + first, RING)
        else:
            z, y = wrap(self.z + first, RING), wrap(self.y + second, RING)
        return self.buf.at[z, y, :, self.part[h]]

    def _exists(self, h, sign, s, pair):
        if s < self.STEPS - 1:
            return True
        if s > self.STEPS - 1:
            return False
        return sign == -1 if h == 0 else (pair < RING // 4) == (sign == 1)

    def _got(self, h, sign, s, pair):
        return self.recv.at[((2 * h + (sign + 1) // 2) * self.STEPS + s) * (RING // 2) + pair]

    def _second(self, h, sign, s, at):
        away = jnp.where(lax.rem(at, 2) == 1, -lax.div(at + 1, 2), lax.div(at, 2))
        place = self._place(h, away, -sign * s)
        got = self._got(h, sign, s, lax.div(at, 2))
        return remote(place, place, self.sent[1][h], got, self._neighbour(h == 1, sign))

    def _wait(self, h, sign, s, pair):
        two = self.buf.at[pl.ds(0, 2), 0, :, self.part[h]]
        got = self._got(h, sign, s, pair)
        remote(two, two, self.sent[1][h], got, self._neighbour(h == 1, sign)).wait_recv()

    def first_step(self, s):
        for h in (0, 1):
            for sign in (1, -1):
                if (1, h, sign, s - 1) in self.copies:
                    self.copies[(1, h, sign, s - 1)].wait_recv()
                if s < (4 if sign == 1 else 3):
                    place = self._place(h, -sign * s, 0)
                    device = self._neighbour(h == 0, sign)
                    self.copies[(1, h, sign, s)] = started(
                        place, place, self.sent[0][h], self.post.slot(), device
                    )

    def begin(self, low, high):
        for at in range(low, high):
            for h in (0, 1):
                for sign in (1, -1):
                    self._second(h, sign, 0, jnp.int32(at)).start()

    def forward(self, low, high):
        def event(n, carry):
            s, pair = 1 + lax.div(n, RING // 2), lax.rem(n, RING // 2)
            for h in (0, 1):
                for sign in (1, -1):
                    self._wait(h, sign, s - 1, pair)
                    for k in (0, 1):
                        self._second(h, sign, s, 2 * pair + k).start()
            return carry

        lax.fori_loop(low, high, event, 0)

    def last(self, pair):
        for h in (0, 1):
            for sign in (1, -1):
                self._wait(h, sign, self.STEPS - 2, pair)
                if self._exists(h, sign, self.STEPS - 1, pair):
                    for k in (0, 1):
                        self._second(h, sign, self.STEPS - 1, jnp.int32(2 * pair + k)).start()

    def finish(self):
        for h in (0, 1):
            for sign in (1, -1):
                for pair in range(RING // 2):
                    if self._exists(h, sign, self.STEPS - 1, pair):
                        self._wait(h, sign, self.STEPS - 1, pair)

    def drain(self):
        for h in (0, 1):
            once = self.buf.at[0, pl.ds(0, RING - 1), :, self.part[h]]
            rows = self.buf.at[pl.ds(0, RING - 1), :, :, self.part[h]]
            for phase, moved in enumerate((once, rows)):
                sent = self.sent[phase][h]
                remote(moved, moved, sent, sent, self._neighbour(True, 1)).wait_send()


def tile(query, pair, tri, shift2, own):
    raw = jnp.dot(query, pair, preferred_element_type=jnp.float32)
    t = raw * (LOG2E * HEAD_DIM**-0.5) - shift2
    spent = jnp.maximum(t, jnp.log(1.0 + jnp.exp2(jnp.minimum(t, 126.0))) * LOG2E)
    taken = t - spent
    if own:
        row = lax.broadcasted_iota(jnp.int32, t.shape, 0)
        col = lax.broadcasted_iota(jnp.int32, t.shape, 1)
        causal = col < row
        spent = jnp.where(causal, spent, 0.0)
    later = jnp.dot(spent.astype(jnp.bfloat16), tri, preferred_element_type=jnp.float32)
    weights = jnp.exp2(taken - later)
    if own:
        weights = jnp.where(causal, weights, 0.0)
    total = jnp.broadcast_to(later[:, :1] + spent[:, :1], (t.shape[0], LANES))
    out = lax.dot_general(
        weights.astype(jnp.bfloat16),
        pair,
        (((1,), (1,)), ((), ())),
        preferred_element_type=jnp.float32,
    )
    return out, total


def rms_scale(v):
    return v * lax.rsqrt(jnp.mean(v * v, axis=-1, keepdims=True) + 1e-06)


def rounded(v):
    return v.astype(jnp.bfloat16).astype(jnp.float32)


def layer_kernel(
    shift_hbm,
    mix_hbm,
    pre_hbm,
    post_hbm,
    conv_gate_hbm,
    conv_up_hbm,
    q_hbm,
    k_hbm,
    v_hbm,
    gate_hbm,
    up_hbm,
    down_hbm,
    resid_hbm,
    wout_hbm,
    result,
    shift_ref,
    gain_mix,
    gain_pre,
    gain_post,
    conv_gate,
    conv_up,
    queries,
    query,
    pairs,
    gate,
    up,
    down,
    whole,
    resid,
    wout,
    tri,
    acc,
    tail,
    attended,
    messages,
    returned,
    mine,
    arrived,
    piece,
    middle,
    edge_out,
    edge_in,
    extended,
    hidden,
    partial,
    partner_partial,
    summed,
    landed,
    passed,
    send,
    recv,
    load,
    edge_sem,
    give_sem,
    take_sem,
    ring_recv,
    early,
):
    sp, tp = lax.axis_index("sp"), lax.axis_index("tp")
    z, y = lax.div(sp, RING), lax.rem(sp, RING)
    x, core = lax.div(tp, 2), lax.rem(tp, 2)
    shards = RING * RING
    span = query.shape[0]
    own_rows = result.shape[0]
    width = gate.shape[1]
    mains = width // LANES
    rest = width - mains * LANES

    loads = [
        pltpu.make_async_copy(a, b, load.at[i])
        for i, (a, b) in enumerate(
            (
                (k_hbm, pairs.at[y, pl.ds(0, HEAD_DIM)]),
                (v_hbm, pairs.at[y, pl.ds(HEAD_DIM, HEAD_DIM)]),
                (q_hbm, queries.at[z]),
                (gate_hbm, gate),
                (up_hbm, up),
                (down_hbm, down),
                (shift_hbm, shift_ref),
                (resid_hbm, resid),
                (wout_hbm, wout),
                (mix_hbm, gain_mix),
                (pre_hbm, gain_pre),
                (post_hbm, gain_post),
                (conv_gate_hbm, conv_gate),
                (conv_up_hbm, conv_up),
            )
        )
    ]
    for copy in loads:
        copy.start()
    barrier = pltpu.get_barrier_semaphore()
    greeted = [{"sp": z * RING + wrap(y + k, RING)} for k in (1, -1)]
    greeted += [{"sp": wrap(z + k, RING) * RING + y} for k in range(1, RING)]
    greeted += [{"sp": wrap(sp + 1, shards)}, {"sp": wrap(sp - 1, shards)}]
    greeted += [{"tp": wrap(tp + k, GROUP)} for k in range(1, GROUP)]
    for device in greeted:
        pl.semaphore_signal(barrier, inc=1, device_id=device, device_id_type=MESH)
    for copy in loads[3:6]:
        copy.wait()
    for j in range(mains):
        here = slice(j * LANES, (j + 1) * LANES)
        whole[z, y, :, 2 * j * LANES : (2 * j + 1) * LANES] = gate[:, here]
        whole[z, y, :, (2 * j + 1) * LANES : (2 * j + 2) * LANES] = up[:, here]
    base = 2 * mains * LANES
    whole[z, y, :, base : base + LANES] = jnp.concatenate(
        [gate[:, mains * LANES :], up[:, mains * LANES :]], axis=1
    )
    down_at = base + LANES
    whole[z, y, :, down_at : down_at + mains * LANES] = down[:, : mains * LANES]
    whole[z, y, :, down_at + mains * LANES :] = jnp.concatenate(
        [down[:, mains * LANES :], jnp.zeros((down.shape[0], LANES - rest), jnp.bfloat16)], axis=1
    )
    for copy in loads[:3]:
        copy.wait()
    pl.semaphore_wait(barrier, len(greeted))

    post = Post(send, recv)

    def key_place(i, part):
        return pairs.at[i] if part is None else pairs.at[i, pl.ds(part * HEAD_DIM, HEAD_DIM)]

    def query_place(i, part):
        half = HEAD_DIM // 2
        return queries.at[i] if part is None else queries.at[i, pl.ds(part * half, half)]

    kv = Line(post, y, key_place, lambda i: {"sp": z * RING + i})
    qs = Line(post, z, query_place, lambda i: {"sp": i * RING + y})
    w = Rings(post, z, y, whole, ring_recv)
    kv.step(0)
    qs.step(0)
    w.first_step(0)
    w.begin(0, 1)

    at = lax.broadcasted_iota(jnp.int32, tri.shape, 0)
    to = lax.broadcasted_iota(jnp.int32, tri.shape, 1)
    tri[...] = jnp.where(at > to, 1.0, 0.0).astype(jnp.bfloat16)
    loads[6].wait()
    shift2 = shift_ref[0] * LOG2E

    def set_query(i):
        padded = jnp.concatenate(
            [queries[i].astype(jnp.float32), jnp.zeros(queries.shape[1:], jnp.float32)], axis=0
        )
        query[...] = padded.T.astype(jnp.bfloat16)

    def visit(first, count, fresh=False):
        found = [
            tile(query[...], pairs[first - k], tri[...], shift2, False) for k in range(count)
        ]
        if fresh:
            total, spent = found.pop(0)
        else:
            total, spent = acc[...], tail[...]
        for out, more in found:
            total = total + jnp.exp2(-spent) * out
            spent = spent + more
        acc[...] = total
        tail[...] = spent

    def report():
        lane = lax.broadcasted_iota(jnp.int32, acc.shape, 1)
        return jnp.where(lane < HEAD_DIM, tail[...], acc[...]).T

    kv.step(1)
    qs.step(1)
    w.first_step(1)
    w.begin(1, 2)
    set_query(z)
    first_out, first_tail = tile(query[...], pairs[y], tri[...], shift2, True)
    acc[...] = first_out
    tail[...] = first_tail
    for s in (2, 3):
        kv.step(s)
        qs.step(s)
        w.first_step(s)
        w.begin(s, s + 1)
    kv.step(4)
    qs.step(4)
    w.first_step(4)
    w.begin(4, 8)

    def one(turn, carry):
        visit(y - 1 - turn, 1)
        return carry

    def several(turn, carry):
        visit(y - 1 - lax.rem(y, UNROLL) - turn * UNROLL, UNROLL)
        return carry

    lax.fori_loop(0, lax.rem(y, UNROLL), one, 0)
    lax.fori_loop(0, lax.div(y, UNROLL), several, 0)
    mine[...] = report()

    def result_copy(i, there):
        return pltpu.make_async_remote_copy(
            src_ref=messages.at[i],
            dst_ref=returned.at[there],
            send_sem=give_sem.at[i],
            recv_sem=take_sem.at[there],
            device_id={"sp": i * RING + y},
            device_id_type=MESH,
        )

    def serve(turn, carry):
        i = z + 1 + turn
        set_query(i)
        visit(RING - 1, UNROLL, fresh=True)
        visit(RING - 1 - UNROLL, UNROLL)
        found = report()
        spent = found[: HEAD_DIM // 8, :]
        high = spent.astype(jnp.bfloat16)
        low = (spent - high.astype(jnp.float32)).astype(jnp.bfloat16)
        messages[i] = jnp.concatenate(
            [found[HEAD_DIM:, :].astype(jnp.bfloat16), high, low], axis=0
        )
        result_copy(i, z).start()
        return carry

    others = RING - 1 - z

    def paced(turn):
        return 1 + lax.div(3 * turn, 4)

    def serve_and_forward(turn, carry):
        serve(turn, carry)
        w.forward(paced(turn), paced(turn + 1))
        return carry

    w.forward(0, 1)
    lax.fori_loop(0, others, serve_and_forward, 0)
    w.forward(paced(others), 7)

    def combine(turn, carry):
        i = z - 1 - turn
        result_copy(i, i).wait_recv()
        spent = mine[:HEAD_DIM, :]
        low_at = HEAD_DIM + HEAD_DIM // 8
        more = returned[i, HEAD_DIM : HEAD_DIM + 1, :].astype(jnp.float32)
        more = more + returned[i, low_at : low_at + 1, :].astype(jnp.float32)
        mine[HEAD_DIM:, :] += jnp.exp2(-spent) * returned[i, :HEAD_DIM, :].astype(jnp.float32)
        mine[:HEAD_DIM, :] = spent + more
        return carry

    lax.fori_loop(0, z, combine, 0)
    sides = jnp.where(core == 0, 1.0, 0.0)
    found = mine[HEAD_DIM:, :]
    attended[...] = jnp.concatenate([found * sides, found * (1.0 - sides)], axis=0).T.astype(
        jnp.bfloat16
    )
    swapped, pieces_in = post.kind(), post.slot()
    for k in range(1, GROUP):
        peer = wrap(tp + k, GROUP)
        rows = pl.ds(pl.multiple_of(peer * own_rows, own_rows), own_rows)
        started(attended.at[rows], arrived.at[tp], swapped, pieces_in, {"tp": peer})
    arrived[tp] = attended[pl.ds(pl.multiple_of(tp * own_rows, own_rows), own_rows), :]
    w.forward(7, 8)
    for copy in loads[7:]:
        copy.wait()
    pieces = arrived.at[pl.ds(0, GROUP - 1)]
    remote(pieces, pieces, swapped, pieces_in, {"tp": wrap(tp + 1, GROUP)}).wait_recv()
    heads = jnp.concatenate([arrived[2 * i] + arrived[2 * i + 1] for i in range(CHIPS)], axis=1)
    mixed = rounded(jnp.dot(heads, wout[...], preferred_element_type=jnp.float32))
    mid = rounded(resid[...].astype(jnp.float32) + gain_mix[...] * rms_scale(mixed))
    middle[...] = mid
    normed = rounded(gain_pre[...] * rms_scale(mid))

    right, left = wrap(x + 1, CHIPS), wrap(x - 1, CHIPS)

    def rows_of(chip, c, half=None):
        start = HALO + (2 * chip + c) * own_rows
        if half is None:
            return piece.at[pl.ds(pl.multiple_of(start, HALO), own_rows)]
        start = start + half * (own_rows // 2)
        return piece.at[pl.ds(pl.multiple_of(start, HALO), own_rows // 2)]

    def to_chip(chip):
        return {"tp": 2 * chip + core}

    partner = {"tp": 2 * x + 1 - core}

    spread_out, crossed = post.kind(), post.slot()

    def move(ref, device):
        return started(ref, ref, spread_out, post.slot(), device)

    def cross(ref):
        started(ref, ref, spread_out, crossed, partner)

    piece[pl.ds(pl.multiple_of(HALO + tp * own_rows, HALO), own_rows), :] = normed.astype(
        jnp.bfloat16
    )
    edge_out[...] = normed[own_rows - (KERNEL - 1) :, :]
    plus = [move(rows_of(x, core, 0), to_chip(right))]
    minus = [move(rows_of(x, core, 1), to_chip(left))]
    plus.append(move(rows_of(x, core, 1), to_chip(right)))
    minus.append(move(rows_of(x, core, 0), to_chip(left)))
    cross(rows_of(x, core))

    def edge_copy(src, device, slot):
        return pltpu.make_async_remote_copy(
            src_ref=src,
            dst_ref=edge_in,
            send_sem=edge_sem.at[slot],
            recv_sem=edge_sem.at[GROUP],
            device_id=device,
            device_id_type=MESH,
        )

    last = tp == GROUP - 1
    ahead = edge_copy(edge_out, {"sp": wrap(sp + 1, shards)}, 0)

    @pl.when(last & (sp < shards - 1))
    def _():
        ahead.start()

    w.last(0)
    plus[0].wait_recv()
    plus.append(move(rows_of(left, core, 0), to_chip(right)))
    cross(rows_of(left, core, 0))
    w.last(1)
    minus[0].wait_recv()
    minus.append(move(rows_of(right, core, 1), to_chip(left)))
    cross(rows_of(right, core, 1))
    w.last(2)
    plus[1].wait_recv()
    cross(rows_of(left, core, 1))
    minus[1].wait_recv()
    cross(rows_of(right, core, 0))
    w.last(3)
    far = wrap(x + 2, CHIPS)
    plus[2].wait_recv()
    cross(rows_of(far, core, 0))
    minus[2].wait_recv()
    cross(rows_of(far, core, 1))

    spread = [edge_copy(edge_in, {"tp": wrap(tp + k, GROUP)}, k) for k in range(1, GROUP)]

    @pl.when(sp > 0)
    def _():
        spread[0].wait_recv()

        @pl.when(last)
        def _():
            for copy in spread:
                copy.start()

    behind = edge_in[...]
    place = lax.broadcasted_iota(jnp.int32, (HALO, piece.shape[1]), 0)
    front = jnp.where(sp > 0, 1, 0)
    filled = jnp.where(
        (place == HALO - 1) & (front == 1),
        behind[1:2, :],
        jnp.where((place == HALO - 2) & (front == 1), behind[0:1, :], 0.0),
    )
    piece[0:HALO, :] = filled.astype(jnp.bfloat16)
    crossings = piece.at[pl.ds(0, GROUP // 2 * own_rows)]
    remote(crossings, crossings, spread_out, crossed, partner).wait_recv()
    depth = piece.shape[1]
    stripe = depth // RING
    ready = (2 * mains + 1 + mains + 1) // 2 // 2
    for j in range(ready):
        found = 0.0
        for d in range(1 - RING // 2, RING // 2):
            near = wrap(z + d, RING)
            found = found + jnp.dot(
                piece[:, pl.ds(pl.multiple_of(near * stripe, stripe), stripe)],
                whole[near, :, :, 2 * j * LANES : (2 * j + 2) * LANES].reshape(stripe, 2 * LANES),
                preferred_element_type=jnp.float32,
            )
        early[j] = found
    w.finish()

    def convolve(low, high, taps):
        rows = partial.shape[0] * own_rows
        found = 0.0
        for tap in range(KERNEL):
            found = found + taps[tap : tap + 1, :] * extended[
                pl.ds(HALO - KERNEL + 1 + tap, rows), low:high
            ]
        return found

    def silu(v):
        return v / (1.0 + jnp.exp(-v))

    for j in range(mains):
        cols = slice(2 * j * LANES, (2 * j + 2) * LANES)
        if j < ready:
            opposite = wrap(z + RING // 2, RING)
            found = early[j] + jnp.dot(
                piece[:, pl.ds(pl.multiple_of(opposite * stripe, stripe), stripe)],
                whole[opposite, :, :, cols].reshape(stripe, 2 * LANES),
                preferred_element_type=jnp.float32,
            )
        else:
            rhs = whole[:, :, :, cols].reshape(depth, 2 * LANES)
            found = jnp.dot(piece[...], rhs, preferred_element_type=jnp.float32)
        extended[...] = rounded(found)
        here = slice(j * LANES, (j + 1) * LANES)
        g = convolve(0, LANES, conv_gate[:, here])
        u = convolve(LANES, 2 * LANES, conv_up[:, here])
        hidden[:, here] = (silu(g) * u).astype(jnp.bfloat16)
    rhs = whole[:, :, :, base : base + LANES].reshape(depth, LANES)
    extended[:, :LANES] = rounded(jnp.dot(piece[...], rhs, preferred_element_type=jnp.float32))
    taps = jnp.concatenate([conv_gate[:, mains * LANES :], conv_up[:, mains * LANES :]], axis=1)
    both = convolve(0, LANES, taps)
    product = silu(both) * pltpu.roll(both, LANES - rest, axis=1)
    inside = lax.broadcasted_iota(jnp.int32, product.shape, 1) < rest
    hidden[:, mains * LANES :] = jnp.where(inside, product, 0.0).astype(jnp.bfloat16)

    wide = depth // 2
    sides_of = [pl.ds(0, wide), pl.ds(wide, wide)]
    halves = (pl.ds(0, own_rows // 2), pl.ds(own_rows // 2, own_rows // 2))
    halved, summing = post.kind(), post.kind()
    swap_in = [post.slot(), post.slot()]
    for part in (0, 1):
        for j in range(part * RING // 2, (part + 1) * RING // 2):
            rhs = whole[j, :, :, down_at:].reshape(stripe, hidden.shape[1])
            found = lax.dot_general(
                hidden[...], rhs, (((1,), (1,)), ((), ())), preferred_element_type=jnp.float32
            )
            partial[:, :, j * stripe : (j + 1) * stripe] = found.astype(jnp.bfloat16).reshape(
                partial.shape[0], own_rows, stripe
            )
        for chip in range(CHIPS):
            started(
                partial.at[2 * chip + 1 - core, :, sides_of[part]],
                partner_partial.at[chip, :, sides_of[part]],
                halved,
                swap_in[part],
                partner,
            )

    def give(src, slot, part, chip):
        there = landed.at[slot, :, sides_of[part]]
        return started(src, there, summing, post.slot(), to_chip(chip))

    got = []
    for part in (0, 1):
        cols = sides_of[part]
        swaps = partner_partial.at[:, :, cols]
        remote(swaps, swaps, halved, swap_in[part], partner).wait_recv()
        for chip in (far, right, left, x):
            summed[chip, :, cols] = (
                partial[2 * chip + core, :, cols].astype(jnp.float32)
                + partner_partial[chip, :, cols].astype(jnp.float32)
            ).astype(jnp.bfloat16)
        got.append(
            [
                give(summed.at[far, halves[0], cols], 0, part, right),
                give(summed.at[far, halves[1], cols], 1, part, left),
                give(summed.at[right, halves[1], cols], 2, part, right),
                give(summed.at[left, halves[0], cols], 3, part, left),
            ]
        )
    kv.drain(pairs.at[pl.ds(0, RING - 1)])
    qs.drain(queries.at[pl.ds(0, RING - 1)])
    w.drain()
    remote(pieces, pieces, swapped, swapped, partner).wait_send()
    moved = piece.at[pl.ds(0, (GROUP - 1) * own_rows)]
    remote(moved, moved, spread_out, spread_out, partner).wait_send()

    def sent(turn, carry):
        result_copy(z + 1 + turn, z).wait_send()
        return carry

    lax.fori_loop(0, others, sent, 0)
    for part in (0, 1):
        cols = sides_of[part]
        for k, (toward, half) in enumerate(((right, 0), (left, 1))):
            got[part][k].wait_recv()
            passed[k, :, cols] = (
                summed[toward, halves[half], cols].astype(jnp.float32)
                + landed[k, :, cols].astype(jnp.float32)
            ).astype(jnp.bfloat16)
            got[part].append(give(passed.at[k, :, cols], 4 + k, part, toward))
    for part in (0, 1):
        for copy in got[part][2:]:
            copy.wait_recv()
    for h, (near, through) in enumerate(((3, 4), (2, 5))):
        ffn = rounded(
            summed[x, halves[h], :].astype(jnp.float32)
            + landed[near].astype(jnp.float32)
            + landed[through].astype(jnp.float32)
        )
        result[halves[h], :] = (
            middle[halves[h], :] + gain_post[...] * rms_scale(ffn)
        ).astype(jnp.bfloat16)

    remote(partner_partial, partner_partial, halved, halved, partner).wait_send()
    remote(landed, landed, summing, summing, partner).wait_send()

    @pl.when(last & (sp < shards - 1))
    def _():
        ahead.wait_send()

    @pl.when(last & (sp > 0))
    def _():
        for copy in spread:
            copy.wait_send()


def local(
    queries,
    keys,
    values,
    score_shift,
    resid,
    w_out,
    gain_mix,
    gain_pre,
    w_gate,
    w_up,
    conv_gate,
    conv_up,
    w_down,
    gain_post,
):
    span = queries.shape[0]
    own_rows, depth = resid.shape
    width = w_gate.shape[1]
    mains = width // LANES
    slab = w_gate.shape[0]
    columns = 2 * mains * LANES + LANES + (mains + 1) * LANES
    vmem = pl.BlockSpec(memory_space=pltpu.VMEM)
    hbm = pl.BlockSpec(memory_space=pltpu.HBM)
    bf16, f32 = jnp.bfloat16, jnp.float32
    return pl.pallas_call(
        layer_kernel,
        out_shape=jax.ShapeDtypeStruct((own_rows, depth), bf16),
        in_specs=[hbm] * 14,
        out_specs=vmem,
        scratch_shapes=[
            pltpu.SMEM((1,), f32),
            pltpu.VMEM((1, depth), f32),
            pltpu.VMEM((1, depth), f32),
            pltpu.VMEM((1, depth), f32),
            pltpu.VMEM(conv_gate.shape, f32),
            pltpu.VMEM(conv_up.shape, f32),
            pltpu.VMEM((RING, HEAD_DIM, span), bf16),
            pltpu.VMEM((span, LANES), bf16),
            pltpu.VMEM((RING, 2 * HEAD_DIM, span), bf16),
            pltpu.VMEM((slab, width), bf16),
            pltpu.VMEM((slab, width), bf16),
            pltpu.VMEM((slab, width), bf16),
            pltpu.VMEM((RING, RING, slab, columns), bf16),
            pltpu.VMEM((own_rows, depth), bf16),
            pltpu.VMEM(w_out.shape, bf16),
            pltpu.VMEM((span, span), bf16),
            pltpu.VMEM((span, LANES), f32),
            pltpu.VMEM((span, LANES), f32),
            pltpu.VMEM((span, LANES), bf16),
            pltpu.VMEM((RING, HEAD_DIM + HEAD_DIM // 4, span), bf16),
            pltpu.VMEM((RING, HEAD_DIM + HEAD_DIM // 4, span), bf16),
            pltpu.VMEM((2 * HEAD_DIM, span), f32),
            pltpu.VMEM((GROUP, own_rows, LANES), bf16),
            pltpu.VMEM((HALO + span, depth), bf16),
            pltpu.VMEM((own_rows, depth), f32),
            pltpu.VMEM((KERNEL - 1, depth), f32),
            pltpu.VMEM((KERNEL - 1, depth), f32),
            pltpu.VMEM((HALO + span, 2 * LANES), f32),
            pltpu.VMEM((span, (mains + 1) * LANES), bf16),
            pltpu.VMEM((GROUP, own_rows, depth), bf16),
            pltpu.VMEM((CHIPS, own_rows, depth), bf16),
            pltpu.VMEM((CHIPS, own_rows, depth), bf16),
            pltpu.VMEM((6, own_rows // 2, depth), bf16),
            pltpu.VMEM((2, own_rows // 2, depth), bf16),
            pltpu.SemaphoreType.DMA((KINDS,)),
            pltpu.SemaphoreType.DMA((ARRIVALS,)),
            pltpu.SemaphoreType.DMA((LOADS,)),
            pltpu.SemaphoreType.DMA((GROUP + 1,)),
            pltpu.SemaphoreType.DMA((RING,)),
            pltpu.SemaphoreType.DMA((RING,)),
            pltpu.SemaphoreType.DMA((RING * RING,)),
            pltpu.VMEM((CHIPS, HALO + span, 2 * LANES), f32),
        ],
        compiler_params=pltpu.CompilerParams(
            collective_id=0, has_side_effects=True, vmem_limit_bytes=67_043_328
        ),
        name="layer",
    )(
        score_shift,
        gain_mix[None],
        gain_pre[None],
        gain_post[None],
        conv_gate,
        conv_up,
        queries.T,
        keys.T,
        values.T,
        w_gate,
        w_up,
        w_down.T,
        resid,
        w_out,
    )


def solution(mesh):
    in_specs = (
        P("sp", "tp"),
        P("sp", "tp"),
        P("sp", "tp"),
        P("tp"),
        P(("sp", "tp"), None),
        P(),
        P(),
        P(),
        P("sp", "tp"),
        P("sp", "tp"),
        P(None, "tp"),
        P(None, "tp"),
        P("tp", "sp"),
        P(),
    )
    out_specs = P(("sp", "tp"), None)
    return jax.shard_map(local, mesh=mesh, in_specs=in_specs, out_specs=out_specs, check_vma=False)
```

```python
import math

import jax
import jax.numpy as jnp
from jax import lax
from jax.experimental import pallas as pl
from jax.experimental.pallas import tpu as pltpu
from jax.sharding import PartitionSpec as P

HEAD_DIM = 64
KERNEL = 3
RING = 8
CHIPS = 4
GROUP = 8
MESH = pl.DeviceIdType.MESH
LOG2E = 1.0 / math.log(2.0)
LANES = 128
HALO = 16
UNROLL = 4
KINDS = 10
ARRIVALS = 45
LOADS = 14


def wrap(v, n):
    return lax.rem(v + 2 * n, n)


class Post:
    def __init__(self, send, recv):
        self.send, self.recv = send, recv
        self.kinds, self.slots = 0, 0

    def kind(self):
        self.kinds += 1
        return self.send.at[self.kinds - 1]

    def slot(self):
        self.slots += 1
        return self.recv.at[self.slots - 1]


def remote(src, dst, sent, got, device):
    return pltpu.make_async_remote_copy(
        src_ref=src,
        dst_ref=dst,
        send_sem=sent,
        recv_sem=got,
        device_id=device,
        device_id_type=MESH,
    )


def started(*arguments):
    copy = remote(*arguments)
    copy.start()
    return copy


class Line:
    def __init__(self, post, me, place, device):
        self.post, self.me, self.place, self.device = post, me, place, device
        self.sent, self.copies = post.kind(), {}

    def step(self, s):
        for sign in (1, -1):
            if (sign, s - 1) in self.copies:
                self.copies[(sign, s - 1)].wait_recv()
            if s < RING // 2:
                part = None if s < RING // 2 - 1 else (0 if sign == 1 else 1)
                ref = self.place(wrap(self.me - sign * s, RING), part)
                device = self.device(wrap(self.me + sign, RING))
                self.copies[(sign, s)] = started(ref, ref, self.sent, self.post.slot(), device)

    def drain(self, whole):
        device = self.device(wrap(self.me + 1, RING))
        remote(whole, whole, self.sent, self.sent, device).wait_send()


class Rings:
    STEPS = RING // 2

    def __init__(self, post, z, y, bufs, recv):
        self.post, self.z, self.y, self.bufs, self.recv = post, z, y, bufs, recv
        self.sent = [[post.kind() for _ in range(2)] for _ in range(2)]
        self.copies = {}

    def _neighbour(self, along_y, sign):
        if along_y:
            return {"sp": self.z * RING + wrap(self.y + sign, RING)}
        return {"sp": wrap(self.z + sign, RING) * RING + self.y}

    def _place(self, h, first, second):
        if h == 0:
            z, y = wrap(self.z + second, RING), wrap(self.y + first, RING)
        else:
            z, y = wrap(self.z + first, RING), wrap(self.y + second, RING)
        return self.bufs[h].at[z, y]

    def _exists(self, h, sign, s, pair):
        if s < self.STEPS - 1:
            return True
        if s > self.STEPS - 1:
            return False
        return (pair < RING // 4) == (sign == 1)

    def _got(self, h, sign, s, pair):
        return self.recv.at[((2 * h + (sign + 1) // 2) * self.STEPS + s) * (RING // 2) + pair]

    def _second(self, h, sign, s, at):
        away = jnp.where(lax.rem(at, 2) == 1, -lax.div(at + 1, 2), lax.div(at, 2))
        place = self._place(h, away, -sign * s)
        got = self._got(h, sign, s, lax.div(at, 2))
        return remote(place, place, self.sent[1][h], got, self._neighbour(h == 1, sign))

    def _wait(self, h, sign, s, pair):
        two = self.bufs[h].at[pl.ds(0, 2), 0]
        got = self._got(h, sign, s, pair)
        remote(two, two, self.sent[1][h], got, self._neighbour(h == 1, sign)).wait_recv()

    def first_step(self, s):
        for h in (0, 1):
            for sign in (1, -1):
                if (1, h, sign, s - 1) in self.copies:
                    self.copies[(1, h, sign, s - 1)].wait_recv()
                if s < (4 if sign == 1 else 3):
                    place = self._place(h, -sign * s, 0)
                    device = self._neighbour(h == 0, sign)
                    self.copies[(1, h, sign, s)] = started(
                        place, place, self.sent[0][h], self.post.slot(), device
                    )

    def begin(self, low, high):
        for at in range(low, high):
            for h in (0, 1):
                for sign in (1, -1):
                    self._second(h, sign, 0, jnp.int32(at)).start()

    def forward(self, low, high):
        def event(n, carry):
            s, pair = 1 + lax.div(n, RING // 2), lax.rem(n, RING // 2)
            for h in (0, 1):
                for sign in (1, -1):
                    self._wait(h, sign, s - 1, pair)
                    for k in (0, 1):
                        self._second(h, sign, s, 2 * pair + k).start()
            return carry

        lax.fori_loop(low, high, event, 0)

    def last(self, pair):
        for h in (0, 1):
            for sign in (1, -1):
                self._wait(h, sign, self.STEPS - 2, pair)
                if self._exists(h, sign, self.STEPS - 1, pair):
                    for k in (0, 1):
                        self._second(h, sign, self.STEPS - 1, jnp.int32(2 * pair + k)).start()

    def finish(self, h):
        for sign in (1, -1):
            for pair in range(RING // 2):
                if self._exists(h, sign, self.STEPS - 1, pair):
                    self._wait(h, sign, self.STEPS - 1, pair)

    def drain(self):
        for h in (0, 1):
            once = self.bufs[h].at[0, pl.ds(0, RING - 1)]
            rows = self.bufs[h].at[pl.ds(0, RING - 1)]
            for phase, moved in enumerate((once, rows)):
                sent = self.sent[phase][h]
                remote(moved, moved, sent, sent, self._neighbour(True, 1)).wait_send()


def tile(query, pair, tri, shift2, own):
    raw = jnp.dot(query, pair, preferred_element_type=jnp.float32)
    t = raw * (LOG2E * HEAD_DIM**-0.5) - shift2
    spent = jnp.maximum(t, jnp.log(1.0 + jnp.exp2(jnp.minimum(t, 126.0))) * LOG2E)
    taken = t - spent
    if own:
        row = lax.broadcasted_iota(jnp.int32, t.shape, 0)
        col = lax.broadcasted_iota(jnp.int32, t.shape, 1)
        causal = col < row
        spent = jnp.where(causal, spent, 0.0)
    later = jnp.dot(spent.astype(jnp.bfloat16), tri, preferred_element_type=jnp.float32)
    weights = jnp.exp2(taken - later)
    if own:
        weights = jnp.where(causal, weights, 0.0)
    total = jnp.broadcast_to(later[:, :1] + spent[:, :1], (t.shape[0], LANES))
    out = lax.dot_general(
        weights.astype(jnp.bfloat16),
        pair,
        (((1,), (1,)), ((), ())),
        preferred_element_type=jnp.float32,
    )
    return out, total


def rms_scale(v):
    return v * lax.rsqrt(jnp.mean(v * v, axis=-1, keepdims=True) + 1e-06)


def rounded(v):
    return v.astype(jnp.bfloat16).astype(jnp.float32)


def layer_kernel(
    shift_hbm,
    mix_hbm,
    pre_hbm,
    post_hbm,
    conv_gate_hbm,
    conv_up_hbm,
    q_hbm,
    k_hbm,
    v_hbm,
    gate_hbm,
    up_hbm,
    down_hbm,
    resid_hbm,
    wout_hbm,
    result,
    shift_ref,
    gain_mix,
    gain_pre,
    gain_post,
    conv_gate,
    conv_up,
    queries,
    query,
    pairs,
    gate,
    up,
    down,
    early_blocks,
    late_blocks,
    resid,
    wout,
    tri,
    acc,
    tail,
    attended,
    messages,
    returned,
    mine,
    arrived,
    piece,
    middle,
    edge_out,
    edge_in,
    extended,
    hidden,
    partial,
    partner_partial,
    summed,
    landed,
    passed,
    send,
    recv,
    load,
    edge_sem,
    give_sem,
    take_sem,
    ring_recv,
    early,
):
    sp, tp = lax.axis_index("sp"), lax.axis_index("tp")
    z, y = lax.div(sp, RING), lax.rem(sp, RING)
    x, core = lax.div(tp, 2), lax.rem(tp, 2)
    shards = RING * RING
    span = query.shape[0]
    own_rows = result.shape[0]
    width = gate.shape[1]
    mains = width // LANES
    rest = width - mains * LANES

    loads = [
        pltpu.make_async_copy(a, b, load.at[i])
        for i, (a, b) in enumerate(
            (
                (k_hbm, pairs.at[y, pl.ds(0, HEAD_DIM)]),
                (v_hbm, pairs.at[y, pl.ds(HEAD_DIM, HEAD_DIM)]),
                (q_hbm, queries.at[z]),
                (gate_hbm, gate),
                (up_hbm, up),
                (down_hbm, down),
                (shift_hbm, shift_ref),
                (resid_hbm, resid),
                (wout_hbm, wout),
                (mix_hbm, gain_mix),
                (pre_hbm, gain_pre),
                (post_hbm, gain_post),
                (conv_gate_hbm, conv_gate),
                (conv_up_hbm, conv_up),
            )
        )
    ]
    barrier = pltpu.get_barrier_semaphore()
    greeted = [{"sp": z * RING + wrap(y + k, RING)} for k in (1, -1)]
    greeted += [{"sp": wrap(z + k, RING) * RING + y} for k in range(1, RING)]
    greeted += [{"sp": wrap(sp + 1, shards)}, {"sp": wrap(sp - 1, shards)}]
    greeted += [{"tp": wrap(tp + k, GROUP)} for k in range(1, GROUP)]
    for device in greeted:
        pl.semaphore_signal(barrier, inc=1, device_id=device, device_id_type=MESH)
    for copy in loads:
        copy.start()
    for copy in loads[:6]:
        copy.wait()
    slab = gate.shape[0]

    def columns(j):
        here = slice(j * LANES, (j + 1) * LANES)
        return [gate[:, here], up[:, here]]

    ends = jnp.concatenate([gate[:, mains * LANES :], up[:, mains * LANES :]], axis=1)
    ready = early_blocks.shape[2] // slab // 2
    for j in range(ready):
        for k, block in enumerate(columns(j)):
            at = (2 * j + k) * slab
            early_blocks[z, y, at : at + slab] = block
    later_blocks = [block for j in range(ready, mains) for block in columns(j)] + [ends]
    down_at = len(later_blocks)
    later_blocks += [down[:, j * LANES : (j + 1) * LANES] for j in range(mains)]
    for k, block in enumerate(later_blocks):
        late_blocks[z, y, k * slab : (k + 1) * slab] = block
    half = slab // 2
    end = down[:, mains * LANES :]
    late_blocks[z, y, len(later_blocks) * slab :] = jnp.concatenate(
        [end[:half], end[half:]], axis=1
    )
    pl.semaphore_wait(barrier, len(greeted))

    post = Post(send, recv)

    def key_place(i, part):
        return pairs.at[i] if part is None else pairs.at[i, pl.ds(part * HEAD_DIM, HEAD_DIM)]

    def query_place(i, part):
        half = HEAD_DIM // 2
        return queries.at[i] if part is None else queries.at[i, pl.ds(part * half, half)]

    kv = Line(post, y, key_place, lambda i: {"sp": z * RING + i})
    qs = Line(post, z, query_place, lambda i: {"sp": i * RING + y})
    w = Rings(post, z, y, (early_blocks, late_blocks), ring_recv)
    kv.step(0)
    qs.step(0)
    w.first_step(0)
    w.begin(0, 1)

    at = lax.broadcasted_iota(jnp.int32, tri.shape, 0)
    to = lax.broadcasted_iota(jnp.int32, tri.shape, 1)
    tri[...] = jnp.where(at > to, 1.0, 0.0).astype(jnp.bfloat16)
    loads[6].wait()
    shift2 = shift_ref[0] * LOG2E

    def set_query(i):
        padded = jnp.concatenate(
            [queries[i].astype(jnp.float32), jnp.zeros(queries.shape[1:], jnp.float32)], axis=0
        )
        query[...] = padded.T.astype(jnp.bfloat16)

    def visit(first, count, fresh=False):
        found = [
            tile(query[...], pairs[first - k], tri[...], shift2, False) for k in range(count)
        ]
        if fresh:
            total, spent = found.pop(0)
        else:
            total, spent = acc[...], tail[...]
        for out, more in found:
            total = total + jnp.exp2(-spent) * out
            spent = spent + more
        acc[...] = total
        tail[...] = spent

    def report():
        lane = lax.broadcasted_iota(jnp.int32, acc.shape, 1)
        return jnp.where(lane < HEAD_DIM, tail[...], acc[...]).T

    kv.step(1)
    qs.step(1)
    w.first_step(1)
    w.begin(1, 2)
    set_query(z)
    first_out, first_tail = tile(query[...], pairs[y], tri[...], shift2, True)
    acc[...] = first_out
    tail[...] = first_tail
    for s in (2, 3):
        kv.step(s)
        qs.step(s)
        w.first_step(s)
        w.begin(s, s + 1)
    kv.step(4)
    qs.step(4)
    w.first_step(4)
    w.begin(4, 8)

    def one(turn, carry):
        visit(y - 1 - turn, 1)
        return carry

    def several(turn, carry):
        visit(y - 1 - lax.rem(y, UNROLL) - turn * UNROLL, UNROLL)
        return carry

    lax.fori_loop(0, lax.rem(y, UNROLL), one, 0)
    lax.fori_loop(0, lax.div(y, UNROLL), several, 0)
    mine[...] = report()

    def result_copy(i, there):
        return pltpu.make_async_remote_copy(
            src_ref=messages.at[i],
            dst_ref=returned.at[there],
            send_sem=give_sem.at[i],
            recv_sem=take_sem.at[there],
            device_id={"sp": i * RING + y},
            device_id_type=MESH,
        )

    def serve(turn, carry):
        i = RING - 1 - turn
        set_query(i)
        visit(RING - 1, UNROLL, fresh=True)
        visit(RING - 1 - UNROLL, UNROLL)
        found = report()
        spent = found[: HEAD_DIM // 8, :]
        high = spent.astype(jnp.bfloat16)
        low = (spent - high.astype(jnp.float32)).astype(jnp.bfloat16)
        messages[i] = jnp.concatenate(
            [found[HEAD_DIM:, :].astype(jnp.bfloat16), high, low], axis=0
        )
        result_copy(i, z).start()
        return carry

    others = RING - 1 - z

    def paced(turn):
        return lax.div(3 * turn, 4)

    def serve_and_forward(turn, carry):
        serve(turn, carry)
        w.forward(paced(turn), paced(turn + 1))
        return carry

    lax.fori_loop(0, others, serve_and_forward, 0)
    w.forward(paced(others), 7)

    def combine(turn, carry):
        i = z - 1 - turn
        result_copy(i, i).wait_recv()
        spent = mine[:HEAD_DIM, :]
        low_at = HEAD_DIM + HEAD_DIM // 8
        more = returned[i, HEAD_DIM : HEAD_DIM + 1, :].astype(jnp.float32)
        more = more + returned[i, low_at : low_at + 1, :].astype(jnp.float32)
        mine[HEAD_DIM:, :] += jnp.exp2(-spent) * returned[i, :HEAD_DIM, :].astype(jnp.float32)
        mine[:HEAD_DIM, :] = spent + more
        return carry

    lax.fori_loop(0, z, combine, 0)
    sides = jnp.where(core == 0, 1.0, 0.0)
    found = mine[HEAD_DIM:, :]
    attended[...] = jnp.concatenate([found * sides, found * (1.0 - sides)], axis=0).T.astype(
        jnp.bfloat16
    )
    swapped, pieces_in = post.kind(), post.slot()
    for k in range(1, GROUP):
        peer = wrap(tp + k, GROUP)
        rows = pl.ds(pl.multiple_of(peer * own_rows, own_rows), own_rows)
        started(attended.at[rows], arrived.at[tp], swapped, pieces_in, {"tp": peer})
    arrived[tp] = attended[pl.ds(pl.multiple_of(tp * own_rows, own_rows), own_rows), :]
    w.forward(7, 8)
    for copy in loads[7:]:
        copy.wait()
    pieces = arrived.at[pl.ds(0, GROUP - 1)]
    remote(pieces, pieces, swapped, pieces_in, {"tp": wrap(tp + 1, GROUP)}).wait_recv()
    heads = jnp.concatenate([arrived[2 * i] + arrived[2 * i + 1] for i in range(CHIPS)], axis=1)
    mixed = rounded(jnp.dot(heads, wout[...], preferred_element_type=jnp.float32))
    mid = rounded(resid[...].astype(jnp.float32) + gain_mix[...] * rms_scale(mixed))
    middle[...] = mid
    normed = rounded(gain_pre[...] * rms_scale(mid))

    right, left = wrap(x + 1, CHIPS), wrap(x - 1, CHIPS)

    def rows_of(chip, c, half=None):
        start = HALO + (2 * chip + c) * own_rows
        if half is None:
            return piece.at[pl.ds(pl.multiple_of(start, HALO), own_rows)]
        start = start + half * (own_rows // 2)
        return piece.at[pl.ds(pl.multiple_of(start, HALO), own_rows // 2)]

    def to_chip(chip):
        return {"tp": 2 * chip + core}

    partner = {"tp": 2 * x + 1 - core}

    spread_out, crossed = post.kind(), post.slot()

    def move(ref, device):
        return started(ref, ref, spread_out, post.slot(), device)

    def cross(ref):
        started(ref, ref, spread_out, crossed, partner)

    piece[pl.ds(pl.multiple_of(HALO + tp * own_rows, HALO), own_rows), :] = normed.astype(
        jnp.bfloat16
    )
    edge_out[...] = normed[own_rows - (KERNEL - 1) :, :]
    plus = [move(rows_of(x, core, 0), to_chip(right))]
    minus = [move(rows_of(x, core, 1), to_chip(left))]
    plus.append(move(rows_of(x, core, 1), to_chip(right)))
    minus.append(move(rows_of(x, core, 0), to_chip(left)))
    cross(rows_of(x, core))

    def edge_copy(src, device, slot):
        return pltpu.make_async_remote_copy(
            src_ref=src,
            dst_ref=edge_in,
            send_sem=edge_sem.at[slot],
            recv_sem=edge_sem.at[GROUP],
            device_id=device,
            device_id_type=MESH,
        )

    last = tp == GROUP - 1
    ahead = edge_copy(edge_out, {"sp": wrap(sp + 1, shards)}, 0)

    @pl.when(last & (sp < shards - 1))
    def _():
        ahead.start()

    w.last(0)
    plus[0].wait_recv()
    plus.append(move(rows_of(left, core, 0), to_chip(right)))
    cross(rows_of(left, core, 0))
    w.last(1)
    minus[0].wait_recv()
    minus.append(move(rows_of(right, core, 1), to_chip(left)))
    cross(rows_of(right, core, 1))
    w.last(2)
    plus[1].wait_recv()
    cross(rows_of(left, core, 1))
    minus[1].wait_recv()
    cross(rows_of(right, core, 0))
    w.last(3)
    far = wrap(x + 2, CHIPS)
    plus[2].wait_recv()
    cross(rows_of(far, core, 0))
    minus[2].wait_recv()
    cross(rows_of(far, core, 1))

    spread = [edge_copy(edge_in, {"tp": wrap(tp + k, GROUP)}, k) for k in range(1, GROUP)]

    @pl.when(sp > 0)
    def _():
        spread[0].wait_recv()

        @pl.when(last)
        def _():
            for copy in spread:
                copy.start()

    behind = edge_in[...]
    place = lax.broadcasted_iota(jnp.int32, (HALO, piece.shape[1]), 0)
    front = jnp.where(sp > 0, 1, 0)
    filled = jnp.where(
        (place == HALO - 1) & (front == 1),
        behind[1:2, :],
        jnp.where((place == HALO - 2) & (front == 1), behind[0:1, :], 0.0),
    )
    piece[0:HALO, :] = filled.astype(jnp.bfloat16)
    crossings = piece.at[pl.ds(0, GROUP // 2 * own_rows)]
    remote(crossings, crossings, spread_out, crossed, partner).wait_recv()
    depth = piece.shape[1]
    stripe = depth // RING

    def slabs(blocks, where, k):
        found = blocks[where, :, k * slab : (k + 1) * slab]
        return found.reshape(RING * slab, LANES)

    def all_slabs(k):
        return late_blocks[:, :, k * slab : (k + 1) * slab].reshape(RING * RING * slab, LANES)

    def pair_product(where, j):
        rhs = jnp.concatenate(
            [slabs(early_blocks, where, 2 * j), slabs(early_blocks, where, 2 * j + 1)], axis=1
        )
        lhs = piece[:, pl.ds(pl.multiple_of(where * stripe, stripe), stripe)]
        return jnp.dot(lhs, rhs, preferred_element_type=jnp.float32)

    for j in range(ready):
        found = 0.0
        for d in range(1 - RING // 2, RING // 2):
            found = found + pair_product(wrap(z + d, RING), j)
        early[j] = found
    w.finish(1)
    w.finish(0)

    def convolve(low, high, taps):
        rows = partial.shape[0] * own_rows
        found = 0.0
        for tap in range(KERNEL):
            found = found + taps[tap : tap + 1, :] * extended[
                pl.ds(HALO - KERNEL + 1 + tap, rows), low:high
            ]
        return found

    def silu(v):
        return v / (1.0 + jnp.exp(-v))

    for j in range(mains):
        if j < ready:
            found = early[j] + pair_product(wrap(z + RING // 2, RING), j)
        else:
            k = 2 * (j - ready)
            rhs = jnp.concatenate([all_slabs(k), all_slabs(k + 1)], axis=1)
            found = jnp.dot(piece[...], rhs, preferred_element_type=jnp.float32)
        extended[...] = rounded(found)
        here = slice(j * LANES, (j + 1) * LANES)
        g = convolve(0, LANES, conv_gate[:, here])
        u = convolve(LANES, 2 * LANES, conv_up[:, here])
        hidden[:, here] = (silu(g) * u).astype(jnp.bfloat16)
    found = jnp.dot(
        piece[...], all_slabs(2 * (mains - ready)), preferred_element_type=jnp.float32
    )
    extended[:, :LANES] = rounded(found)
    taps = jnp.concatenate([conv_gate[:, mains * LANES :], conv_up[:, mains * LANES :]], axis=1)
    both = convolve(0, LANES, taps)
    product = silu(both) * pltpu.roll(both, LANES - rest, axis=1)
    inside = lax.broadcasted_iota(jnp.int32, product.shape, 1) < rest
    hidden[:, mains * LANES :] = jnp.where(inside, product, 0.0).astype(jnp.bfloat16)

    wide = depth // 2
    sides_of = [pl.ds(0, wide), pl.ds(wide, wide)]
    halves = (pl.ds(0, own_rows // 2), pl.ds(own_rows // 2, own_rows // 2))
    halved, summing = post.kind(), post.kind()
    swap_in = [post.slot(), post.slot()]
    for part in (0, 1):
        for j in range(part * RING // 2, (part + 1) * RING // 2):
            end = late_blocks[j, :, len(later_blocks) * slab :].astype(jnp.float32)
            end = end.reshape(RING * half, LANES)
            inside = lax.broadcasted_iota(jnp.int32, end.shape, 1) < rest
            ends = [
                jnp.where(inside, v, 0.0).astype(jnp.bfloat16).reshape(RING, half, LANES)
                for v in (end, pltpu.roll(end, LANES - rest, axis=1))
            ]
            rhs = jnp.concatenate(
                [slabs(late_blocks, j, down_at + k) for k in range(mains)]
                + [jnp.concatenate(ends, axis=1).reshape(stripe, LANES)],
                axis=1,
            )
            found = lax.dot_general(
                hidden[...], rhs, (((1,), (1,)), ((), ())), preferred_element_type=jnp.float32
            )
            partial[:, :, j * stripe : (j + 1) * stripe] = found.astype(jnp.bfloat16).reshape(
                partial.shape[0], own_rows, stripe
            )
        for chip in range(CHIPS):
            started(
                partial.at[2 * chip + 1 - core, :, sides_of[part]],
                partner_partial.at[chip, :, sides_of[part]],
                halved,
                swap_in[part],
                partner,
            )

    ends_in = post.slot()

    def give(src, slot, part, chip):
        there = landed.at[slot, :, sides_of[part]]
        arrival = post.slot() if slot < 2 else ends_in
        return started(src, there, summing, arrival, to_chip(chip))

    got = []
    for part in (0, 1):
        cols = sides_of[part]
        swaps = partner_partial.at[:, :, cols]
        remote(swaps, swaps, halved, swap_in[part], partner).wait_recv()
        for chip in (far, right, left, x):
            summed[chip, :, cols] = (
                partial[2 * chip + core, :, cols].astype(jnp.float32)
                + partner_partial[chip, :, cols].astype(jnp.float32)
            ).astype(jnp.bfloat16)
        got.append(
            [
                give(summed.at[far, halves[0], cols], 0, part, right),
                give(summed.at[far, halves[1], cols], 1, part, left),
                give(summed.at[right, halves[1], cols], 2, part, right),
                give(summed.at[left, halves[0], cols], 3, part, left),
            ]
        )
    kv.drain(pairs.at[pl.ds(0, RING - 1)])
    qs.drain(queries.at[pl.ds(0, RING - 1)])
    w.drain()
    remote(pieces, pieces, swapped, swapped, partner).wait_send()
    moved = piece.at[pl.ds(0, (GROUP - 1) * own_rows)]
    remote(moved, moved, spread_out, spread_out, partner).wait_send()

    def sent(turn, carry):
        result_copy(z + 1 + turn, z).wait_send()
        return carry

    lax.fori_loop(0, others, sent, 0)
    for part in (0, 1):
        cols = sides_of[part]
        for k, (toward, half) in enumerate(((right, 0), (left, 1))):
            got[part][k].wait_recv()
            passed[k, :, cols] = (
                summed[toward, halves[half], cols].astype(jnp.float32)
                + landed[k, :, cols].astype(jnp.float32)
            ).astype(jnp.bfloat16)
            give(passed.at[k, :, cols], 4 + k, part, toward)
    ending = landed.at[pl.ds(2, 4)]
    remote(ending, ending, summing, ends_in, partner).wait_recv()
    for h, (near, through) in enumerate(((3, 4), (2, 5))):
        ffn = rounded(
            summed[x, halves[h], :].astype(jnp.float32)
            + landed[near].astype(jnp.float32)
            + landed[through].astype(jnp.float32)
        )
        result[halves[h], :] = (
            middle[halves[h], :] + gain_post[...] * rms_scale(ffn)
        ).astype(jnp.bfloat16)

    remote(partner_partial, partner_partial, halved, halved, partner).wait_send()
    remote(landed, landed, summing, summing, partner).wait_send()

    @pl.when(last & (sp < shards - 1))
    def _():
        ahead.wait_send()

    @pl.when(last & (sp > 0))
    def _():
        for copy in spread:
            copy.wait_send()


def local(
    queries,
    keys,
    values,
    score_shift,
    resid,
    w_out,
    gain_mix,
    gain_pre,
    w_gate,
    w_up,
    conv_gate,
    conv_up,
    w_down,
    gain_post,
):
    span = queries.shape[0]
    own_rows, depth = resid.shape
    width = w_gate.shape[1]
    mains = width // LANES
    slab = w_gate.shape[0]
    tiles = 3 * mains + 1
    early_tiles = tiles // 4 * 2
    vmem = pl.BlockSpec(memory_space=pltpu.VMEM)
    hbm = pl.BlockSpec(memory_space=pltpu.HBM)
    bf16, f32 = jnp.bfloat16, jnp.float32
    return pl.pallas_call(
        layer_kernel,
        out_shape=jax.ShapeDtypeStruct((own_rows, depth), bf16),
        in_specs=[hbm] * 14,
        out_specs=vmem,
        scratch_shapes=[
            pltpu.SMEM((1,), f32),
            pltpu.VMEM((1, depth), f32),
            pltpu.VMEM((1, depth), f32),
            pltpu.VMEM((1, depth), f32),
            pltpu.VMEM(conv_gate.shape, f32),
            pltpu.VMEM(conv_up.shape, f32),
            pltpu.VMEM((RING, HEAD_DIM, span), bf16),
            pltpu.VMEM((span, LANES), bf16),
            pltpu.VMEM((RING, 2 * HEAD_DIM, span), bf16),
            pltpu.VMEM((slab, width), bf16),
            pltpu.VMEM((slab, width), bf16),
            pltpu.VMEM((slab, width), bf16),
            pltpu.VMEM((RING, RING, early_tiles * slab, LANES), bf16),
            pltpu.VMEM((RING, RING, (tiles - early_tiles) * slab + slab // 2, LANES), bf16),
            pltpu.VMEM((own_rows, depth), bf16),
            pltpu.VMEM(w_out.shape, bf16),
            pltpu.VMEM((span, span), bf16),
            pltpu.VMEM((span, LANES), f32),
            pltpu.VMEM((span, LANES), f32),
            pltpu.VMEM((span, LANES), bf16),
            pltpu.VMEM((RING, HEAD_DIM + HEAD_DIM // 4, span), bf16),
            pltpu.VMEM((RING, HEAD_DIM + HEAD_DIM // 4, span), bf16),
            pltpu.VMEM((2 * HEAD_DIM, span), f32),
            pltpu.VMEM((GROUP, own_rows, LANES), bf16),
            pltpu.VMEM((HALO + span, depth), bf16),
            pltpu.VMEM((own_rows, depth), f32),
            pltpu.VMEM((KERNEL - 1, depth), f32),
            pltpu.VMEM((KERNEL - 1, depth), f32),
            pltpu.VMEM((HALO + span, 2 * LANES), f32),
            pltpu.VMEM((span, (mains + 1) * LANES), bf16),
            pltpu.VMEM((GROUP, own_rows, depth), bf16),
            pltpu.VMEM((CHIPS, own_rows, depth), bf16),
            pltpu.VMEM((CHIPS, own_rows, depth), bf16),
            pltpu.VMEM((6, own_rows // 2, depth), bf16),
            pltpu.VMEM((2, own_rows // 2, depth), bf16),
            pltpu.SemaphoreType.DMA((KINDS,)),
            pltpu.SemaphoreType.DMA((ARRIVALS,)),
            pltpu.SemaphoreType.DMA((LOADS,)),
            pltpu.SemaphoreType.DMA((GROUP + 1,)),
            pltpu.SemaphoreType.DMA((RING,)),
            pltpu.SemaphoreType.DMA((RING,)),
            pltpu.SemaphoreType.DMA((RING * RING,)),
            pltpu.VMEM((early_tiles // 2, HALO + span, 2 * LANES), f32),
        ],
        compiler_params=pltpu.CompilerParams(
            collective_id=0, has_side_effects=True, vmem_limit_bytes=67_043_328
        ),
        name="layer",
    )(
        score_shift,
        gain_mix[None],
        gain_pre[None],
        gain_post[None],
        conv_gate,
        conv_up,
        queries.T,
        keys.T,
        values.T,
        w_gate,
        w_up,
        w_down.T,
        resid,
        w_out,
    )


def solution(mesh):
    in_specs = (
        P("sp", "tp"),
        P("sp", "tp"),
        P("sp", "tp"),
        P("tp"),
        P(("sp", "tp"), None),
        P(),
        P(),
        P(),
        P("sp", "tp"),
        P("sp", "tp"),
        P(None, "tp"),
        P(None, "tp"),
        P("tp", "sp"),
        P(),
    )
    out_specs = P(("sp", "tp"), None)
    return jax.shard_map(local, mesh=mesh, in_specs=in_specs, out_specs=out_specs, check_vma=False)
```

```python
import math

import jax
import jax.numpy as jnp
from jax import lax
from jax.experimental import pallas as pl
from jax.experimental.pallas import tpu as pltpu
from jax.sharding import PartitionSpec as P

HEAD_DIM = 64
KERNEL = 3
RING = 8
CHIPS = 4
GROUP = 8
MESH = pl.DeviceIdType.MESH
LOG2E = 1.0 / math.log(2.0)
LANES = 128
HALO = 16
UNROLL = 4
KINDS = 10
ARRIVALS = 31
LOADS = 14


def wrap(v, n):
    return lax.rem(v + 2 * n, n)


class Post:
    def __init__(self, send, recv):
        self.send, self.recv = send, recv
        self.kinds, self.slots = 0, 0

    def kind(self):
        self.kinds += 1
        return self.send.at[self.kinds - 1]

    def slot(self):
        self.slots += 1
        return self.recv.at[self.slots - 1]


def remote(src, dst, sent, got, device):
    return pltpu.make_async_remote_copy(
        src_ref=src,
        dst_ref=dst,
        send_sem=sent,
        recv_sem=got,
        device_id=device,
        device_id_type=MESH,
    )


def started(*arguments):
    copy = remote(*arguments)
    copy.start()
    return copy


class Line:
    STEPS = RING // 2

    def __init__(self, post, me, buf, place, device):
        self.me, self.buf, self.place, self.device = me, buf, place, device
        self.sent = post.kind()
        self.got = [post.slot() for _ in range(self.STEPS)]

    def _settle(self, ref, got):
        return remote(ref, ref, self.sent, got, self.device(wrap(self.me + 1, RING)))

    def step(self, s):
        if s > 0:
            count = 2 if s < self.STEPS else 1
            self._settle(self.buf.at[pl.ds(0, count)], self.got[s - 1]).wait_recv()
        if s < self.STEPS:
            for sign in (1, -1):
                part = None if s < self.STEPS - 1 else (0 if sign == 1 else 1)
                ref = self.place(wrap(self.me - sign * s, RING), part)
                device = self.device(wrap(self.me + sign, RING))
                started(ref, ref, self.sent, self.got[s], device)

    def drain(self):
        self._settle(self.buf.at[pl.ds(0, RING - 1)], self.sent).wait_send()


class Rings:
    STEPS = RING // 2

    def __init__(self, post, z, y, bufs, recv):
        self.z, self.y, self.bufs, self.recv = z, y, bufs, recv
        self.sent = [[post.kind() for _ in range(2)] for _ in range(2)]
        self.got = [[post.slot() for _ in range(self.STEPS)] for _ in range(2)]

    def _neighbour(self, along_y, sign):
        if along_y:
            return {"sp": self.z * RING + wrap(self.y + sign, RING)}
        return {"sp": wrap(self.z + sign, RING) * RING + self.y}

    def _place(self, h, first, second):
        if h == 0:
            z, y = wrap(self.z + second, RING), wrap(self.y + first, RING)
        else:
            z, y = wrap(self.z + first, RING), wrap(self.y + second, RING)
        return self.bufs[h].at[z, y]

    def _got(self, h, s, pair):
        return self.recv.at[(h * self.STEPS + s) * (RING // 2) + pair]

    def _second(self, h, sign, s, at):
        away = jnp.where(lax.rem(at, 2) == 1, -lax.div(at + 1, 2), lax.div(at, 2))
        place = self._place(h, away, -sign * s)
        got = self._got(h, s, lax.div(at, 2))
        return remote(place, place, self.sent[1][h], got, self._neighbour(h == 1, sign))

    def _wait(self, h, s, pair, sides=2):
        blocks = self.bufs[h].at[pl.ds(0, 2 * sides), 0]
        got = self._got(h, s, pair)
        remote(blocks, blocks, self.sent[1][h], got, self._neighbour(h == 1, 1)).wait_recv()

    def first_step(self, s):
        for h in (0, 1):
            if s > 0:
                blocks = self.bufs[h].at[0, pl.ds(0, 2 if s < self.STEPS else 1)]
                device = self._neighbour(h == 0, 1)
                remote(blocks, blocks, self.sent[0][h], self.got[h][s - 1], device).wait_recv()
            for sign in (1, -1):
                if s < (self.STEPS if sign == 1 else self.STEPS - 1):
                    place = self._place(h, -sign * s, 0)
                    device = self._neighbour(h == 0, sign)
                    started(place, place, self.sent[0][h], self.got[h][s], device)

    def begin(self, low, high):
        for at in range(low, high):
            for h in (0, 1):
                for sign in (1, -1):
                    self._second(h, sign, 0, jnp.int32(at)).start()

    def forward(self, low, high):
        def event(n, carry):
            s, pair = 1 + lax.div(n, RING // 2), lax.rem(n, RING // 2)
            for h in (0, 1):
                self._wait(h, s - 1, pair)
                for k in (0, 1):
                    for sign in (1, -1):
                        self._second(h, sign, s, 2 * pair + k).start()
            return carry

        lax.fori_loop(low, high, event, 0)

    def last(self, pair):
        sign = 1 if pair < RING // 4 else -1
        for h in (0, 1):
            self._wait(h, self.STEPS - 2, pair)
            for k in (0, 1):
                self._second(h, sign, self.STEPS - 1, jnp.int32(2 * pair + k)).start()

    def finish(self, h):
        for pair in range(RING // 2):
            self._wait(h, self.STEPS - 1, pair, 1)

    def drain(self):
        for h in (0, 1):
            once = self.bufs[h].at[0, pl.ds(0, RING - 1)]
            rows = self.bufs[h].at[pl.ds(0, RING - 1)]
            for phase, moved in enumerate((once, rows)):
                sent = self.sent[phase][h]
                remote(moved, moved, sent, sent, self._neighbour(True, 1)).wait_send()


def tile(query, pair, tri, shift2, own):
    raw = jnp.dot(query, pair, preferred_element_type=jnp.float32)
    t = raw * (LOG2E * HEAD_DIM**-0.5) - shift2
    spent = jnp.maximum(t, jnp.log(1.0 + jnp.exp2(jnp.minimum(t, 126.0))) * LOG2E)
    taken = t - spent
    if own:
        row = lax.broadcasted_iota(jnp.int32, t.shape, 0)
        col = lax.broadcasted_iota(jnp.int32, t.shape, 1)
        causal = col < row
        spent = jnp.where(causal, spent, 0.0)
    later = jnp.dot(spent.astype(jnp.bfloat16), tri, preferred_element_type=jnp.float32)
    weights = jnp.exp2(taken - later)
    if own:
        weights = jnp.where(causal, weights, 0.0)
    total = jnp.broadcast_to(later[:, :1] + spent[:, :1], (t.shape[0], LANES))
    out = lax.dot_general(
        weights.astype(jnp.bfloat16),
        pair,
        (((1,), (1,)), ((), ())),
        preferred_element_type=jnp.float32,
    )
    return out, total


def rms_scale(v):
    return v * lax.rsqrt(jnp.mean(v * v, axis=-1, keepdims=True) + 1e-06)


def rounded(v):
    return v.astype(jnp.bfloat16).astype(jnp.float32)


def layer_kernel(
    shift_hbm,
    mix_hbm,
    pre_hbm,
    post_hbm,
    conv_gate_hbm,
    conv_up_hbm,
    q_hbm,
    k_hbm,
    v_hbm,
    gate_hbm,
    up_hbm,
    down_hbm,
    resid_hbm,
    wout_hbm,
    result,
    shift_ref,
    gain_mix,
    gain_pre,
    gain_post,
    conv_gate,
    conv_up,
    queries,
    query,
    pairs,
    gate,
    up,
    down,
    early_blocks,
    late_blocks,
    resid,
    wout,
    tri,
    acc,
    tail,
    attended,
    messages,
    returned,
    mine,
    arrived,
    piece,
    middle,
    edge_out,
    edge_in,
    extended,
    hidden,
    partial,
    partner_partial,
    summed,
    landed,
    passed,
    send,
    recv,
    load,
    edge_sem,
    give_sem,
    take_sem,
    ring_recv,
    early,
):
    sp, tp = lax.axis_index("sp"), lax.axis_index("tp")
    z, y = lax.div(sp, RING), lax.rem(sp, RING)
    x, core = lax.div(tp, 2), lax.rem(tp, 2)
    shards = RING * RING
    span = query.shape[0]
    own_rows = result.shape[0]
    width = gate.shape[1]
    mains = width // LANES
    rest = width - mains * LANES

    loads = [
        pltpu.make_async_copy(a, b, load.at[i])
        for i, (a, b) in enumerate(
            (
                (k_hbm, pairs.at[y, pl.ds(0, HEAD_DIM)]),
                (v_hbm, pairs.at[y, pl.ds(HEAD_DIM, HEAD_DIM)]),
                (q_hbm, queries.at[z]),
                (gate_hbm, gate),
                (up_hbm, up),
                (down_hbm, down),
                (shift_hbm, shift_ref),
                (resid_hbm, resid),
                (wout_hbm, wout),
                (mix_hbm, gain_mix),
                (pre_hbm, gain_pre),
                (post_hbm, gain_post),
                (conv_gate_hbm, conv_gate),
                (conv_up_hbm, conv_up),
            )
        )
    ]
    barrier = pltpu.get_barrier_semaphore()
    greeted = [{"sp": z * RING + wrap(y + k, RING)} for k in (1, -1)]
    greeted += [{"sp": wrap(z + k, RING) * RING + y} for k in range(1, RING)]
    greeted += [{"sp": wrap(sp + 1, shards)}, {"sp": wrap(sp - 1, shards)}]
    greeted += [{"tp": wrap(tp + k, GROUP)} for k in range(1, GROUP)]
    for device in greeted:
        pl.semaphore_signal(barrier, inc=1, device_id=device, device_id_type=MESH)
    for copy in loads:
        copy.start()
    for copy in loads[:6]:
        copy.wait()
    slab = gate.shape[0]

    def columns(j):
        here = slice(j * LANES, (j + 1) * LANES)
        return [gate[:, here], up[:, here]]

    ends = jnp.concatenate([gate[:, mains * LANES :], up[:, mains * LANES :]], axis=1)
    ready = early_blocks.shape[2] // slab // 2
    for j in range(ready):
        for k, block in enumerate(columns(j)):
            at = (2 * j + k) * slab
            early_blocks[z, y, at : at + slab] = block
    later_blocks = [block for j in range(ready, mains) for block in columns(j)] + [ends]
    down_at = len(later_blocks)
    later_blocks += [down[:, j * LANES : (j + 1) * LANES] for j in range(mains)]
    for k, block in enumerate(later_blocks):
        late_blocks[z, y, k * slab : (k + 1) * slab] = block
    half = slab // 2
    end = down[:, mains * LANES :]
    late_blocks[z, y, len(later_blocks) * slab :] = jnp.concatenate(
        [end[:half], end[half:]], axis=1
    )
    pl.semaphore_wait(barrier, len(greeted))

    post = Post(send, recv)

    def key_place(i, part):
        return pairs.at[i] if part is None else pairs.at[i, pl.ds(part * HEAD_DIM, HEAD_DIM)]

    def query_place(i, part):
        half = HEAD_DIM // 2
        return queries.at[i] if part is None else queries.at[i, pl.ds(part * half, half)]

    kv = Line(post, y, pairs, key_place, lambda i: {"sp": z * RING + i})
    qs = Line(post, z, queries, query_place, lambda i: {"sp": i * RING + y})
    w = Rings(post, z, y, (early_blocks, late_blocks), ring_recv)
    kv.step(0)
    qs.step(0)
    w.first_step(0)
    w.begin(0, 1)

    at = lax.broadcasted_iota(jnp.int32, tri.shape, 0)
    to = lax.broadcasted_iota(jnp.int32, tri.shape, 1)
    tri[...] = jnp.where(at > to, 1.0, 0.0).astype(jnp.bfloat16)
    loads[6].wait()
    shift2 = shift_ref[0] * LOG2E

    def set_query(i):
        padded = jnp.concatenate(
            [queries[i].astype(jnp.float32), jnp.zeros(queries.shape[1:], jnp.float32)], axis=0
        )
        query[...] = padded.T.astype(jnp.bfloat16)

    def visit(first, count, fresh=False):
        found = [
            tile(query[...], pairs[first - k], tri[...], shift2, False) for k in range(count)
        ]
        if fresh:
            total, spent = found.pop(0)
        else:
            total, spent = acc[...], tail[...]
        for out, more in found:
            total = total + jnp.exp2(-spent) * out
            spent = spent + more
        acc[...] = total
        tail[...] = spent

    def report():
        lane = lax.broadcasted_iota(jnp.int32, acc.shape, 1)
        return jnp.where(lane < HEAD_DIM, tail[...], acc[...]).T

    kv.step(1)
    qs.step(1)
    w.first_step(1)
    w.begin(1, 2)
    set_query(z)
    first_out, first_tail = tile(query[...], pairs[y], tri[...], shift2, True)
    acc[...] = first_out
    tail[...] = first_tail
    for s in (2, 3):
        kv.step(s)
        qs.step(s)
        w.first_step(s)
        w.begin(s, s + 1)
    kv.step(4)
    qs.step(4)
    w.first_step(4)
    w.begin(4, 8)

    def one(turn, carry):
        visit(y - 1 - turn, 1)
        return carry

    def several(turn, carry):
        visit(y - 1 - lax.rem(y, UNROLL) - turn * UNROLL, UNROLL)
        return carry

    lax.fori_loop(0, lax.rem(y, UNROLL), one, 0)
    lax.fori_loop(0, lax.div(y, UNROLL), several, 0)
    mine[...] = report()

    def result_copy(i, there):
        return pltpu.make_async_remote_copy(
            src_ref=messages.at[i],
            dst_ref=returned.at[there],
            send_sem=give_sem.at[i],
            recv_sem=take_sem.at[there],
            device_id={"sp": i * RING + y},
            device_id_type=MESH,
        )

    def serve(turn, carry):
        i = RING - 1 - turn
        set_query(i)
        visit(RING - 1, RING, fresh=True)
        found = report()
        spent = found[: HEAD_DIM // 8, :]
        high = spent.astype(jnp.bfloat16)
        low = (spent - high.astype(jnp.float32)).astype(jnp.bfloat16)
        messages[i] = jnp.concatenate(
            [found[HEAD_DIM:, :].astype(jnp.bfloat16), high, low], axis=0
        )
        result_copy(i, z).start()
        return carry

    others = RING - 1 - z

    def paced(turn):
        return lax.div(3 * turn, 4)

    def serve_and_forward(turn, carry):
        serve(turn, carry)
        w.forward(paced(turn), paced(turn + 1))
        return carry

    lax.fori_loop(0, others, serve_and_forward, 0)
    w.forward(paced(others), 7)

    def combine(turn, carry):
        i = z - 1 - turn
        result_copy(i, i).wait_recv()
        spent = mine[:HEAD_DIM, :]
        low_at = HEAD_DIM + HEAD_DIM // 8
        more = returned[i, HEAD_DIM : HEAD_DIM + 1, :].astype(jnp.float32)
        more = more + returned[i, low_at : low_at + 1, :].astype(jnp.float32)
        mine[HEAD_DIM:, :] += jnp.exp2(-spent) * returned[i, :HEAD_DIM, :].astype(jnp.float32)
        mine[:HEAD_DIM, :] = spent + more
        return carry

    lax.fori_loop(0, z, combine, 0)
    sides = jnp.where(core == 0, 1.0, 0.0)
    found = mine[HEAD_DIM:, :]
    attended[...] = jnp.concatenate([found * sides, found * (1.0 - sides)], axis=0).T.astype(
        jnp.bfloat16
    )
    swapped, pieces_in = post.kind(), post.slot()
    for k in range(1, GROUP):
        peer = wrap(tp + k, GROUP)
        rows = pl.ds(pl.multiple_of(peer * own_rows, own_rows), own_rows)
        started(attended.at[rows], arrived.at[tp], swapped, pieces_in, {"tp": peer})
    arrived[tp] = attended[pl.ds(pl.multiple_of(tp * own_rows, own_rows), own_rows), :]
    w.forward(7, 8)
    for copy in loads[7:]:
        copy.wait()
    pieces = arrived.at[pl.ds(0, GROUP - 1)]
    remote(pieces, pieces, swapped, pieces_in, {"tp": wrap(tp + 1, GROUP)}).wait_recv()
    heads = jnp.concatenate([arrived[2 * i] + arrived[2 * i + 1] for i in range(CHIPS)], axis=1)
    mixed = rounded(jnp.dot(heads, wout[...], preferred_element_type=jnp.float32))
    mid = rounded(resid[...].astype(jnp.float32) + gain_mix[...] * rms_scale(mixed))
    middle[...] = mid
    normed = rounded(gain_pre[...] * rms_scale(mid))

    right, left = wrap(x + 1, CHIPS), wrap(x - 1, CHIPS)

    def rows_of(chip, c, half=None):
        start = HALO + (2 * chip + c) * own_rows
        if half is None:
            return piece.at[pl.ds(pl.multiple_of(start, HALO), own_rows)]
        start = start + half * (own_rows // 2)
        return piece.at[pl.ds(pl.multiple_of(start, HALO), own_rows // 2)]

    def to_chip(chip):
        return {"tp": 2 * chip + core}

    partner = {"tp": 2 * x + 1 - core}

    spread_out, crossed = post.kind(), post.slot()

    def move(ref, device):
        return started(ref, ref, spread_out, post.slot(), device)

    def cross(ref):
        started(ref, ref, spread_out, crossed, partner)

    piece[pl.ds(pl.multiple_of(HALO + tp * own_rows, HALO), own_rows), :] = normed.astype(
        jnp.bfloat16
    )
    edge_out[...] = normed[own_rows - (KERNEL - 1) :, :]
    plus = [move(rows_of(x, core, 0), to_chip(right))]
    minus = [move(rows_of(x, core, 1), to_chip(left))]
    plus.append(move(rows_of(x, core, 1), to_chip(right)))
    minus.append(move(rows_of(x, core, 0), to_chip(left)))
    cross(rows_of(x, core))

    def edge_copy(src, device, slot):
        return pltpu.make_async_remote_copy(
            src_ref=src,
            dst_ref=edge_in,
            send_sem=edge_sem.at[slot],
            recv_sem=edge_sem.at[GROUP],
            device_id=device,
            device_id_type=MESH,
        )

    last = tp == GROUP - 1
    ahead = edge_copy(edge_out, {"sp": wrap(sp + 1, shards)}, 0)

    @pl.when(last & (sp < shards - 1))
    def _():
        ahead.start()

    w.last(0)
    plus[0].wait_recv()
    plus.append(move(rows_of(left, core, 0), to_chip(right)))
    cross(rows_of(left, core, 0))
    w.last(1)
    minus[0].wait_recv()
    minus.append(move(rows_of(right, core, 1), to_chip(left)))
    cross(rows_of(right, core, 1))
    w.last(2)
    plus[1].wait_recv()
    cross(rows_of(left, core, 1))
    minus[1].wait_recv()
    cross(rows_of(right, core, 0))
    w.last(3)
    far = wrap(x + 2, CHIPS)
    plus[2].wait_recv()
    cross(rows_of(far, core, 0))
    minus[2].wait_recv()
    cross(rows_of(far, core, 1))

    spread = [edge_copy(edge_in, {"tp": wrap(tp + k, GROUP)}, k) for k in range(1, GROUP)]

    @pl.when(sp > 0)
    def _():
        spread[0].wait_recv()

        @pl.when(last)
        def _():
            for copy in spread:
                copy.start()

    behind = edge_in[...]
    place = lax.broadcasted_iota(jnp.int32, (HALO, piece.shape[1]), 0)
    front = jnp.where(sp > 0, 1, 0)
    filled = jnp.where(
        (place == HALO - 1) & (front == 1),
        behind[1:2, :],
        jnp.where((place == HALO - 2) & (front == 1), behind[0:1, :], 0.0),
    )
    piece[0:HALO, :] = filled.astype(jnp.bfloat16)
    crossings = piece.at[pl.ds(0, GROUP // 2 * own_rows)]
    remote(crossings, crossings, spread_out, crossed, partner).wait_recv()
    depth = piece.shape[1]
    stripe = depth // RING

    def slabs(blocks, where, k):
        found = blocks[where, :, k * slab : (k + 1) * slab]
        return found.reshape(RING * slab, LANES)

    def all_slabs(k):
        return late_blocks[:, :, k * slab : (k + 1) * slab].reshape(RING * RING * slab, LANES)

    def pair_product(where, j):
        rhs = jnp.concatenate(
            [slabs(early_blocks, where, 2 * j), slabs(early_blocks, where, 2 * j + 1)], axis=1
        )
        lhs = piece[:, pl.ds(pl.multiple_of(where * stripe, stripe), stripe)]
        return jnp.dot(lhs, rhs, preferred_element_type=jnp.float32)

    for j in range(ready):
        found = 0.0
        for d in range(1 - RING // 2, RING // 2):
            found = found + pair_product(wrap(z + d, RING), j)
        early[j] = found
    w.finish(1)

    def convolve(low, high, taps):
        rows = partial.shape[0] * own_rows
        found = 0.0
        for tap in range(KERNEL):
            found = found + taps[tap : tap + 1, :] * extended[
                pl.ds(HALO - KERNEL + 1 + tap, rows), low:high
            ]
        return found

    def silu(v):
        return v / (1.0 + jnp.exp(-v))

    def gated(j, found):
        extended[...] = rounded(found)
        here = slice(j * LANES, (j + 1) * LANES)
        g = convolve(0, LANES, conv_gate[:, here])
        u = convolve(LANES, 2 * LANES, conv_up[:, here])
        hidden[:, here] = (silu(g) * u).astype(jnp.bfloat16)

    for j in range(ready, mains):
        k = 2 * (j - ready)
        rhs = jnp.concatenate([all_slabs(k), all_slabs(k + 1)], axis=1)
        gated(j, jnp.dot(piece[...], rhs, preferred_element_type=jnp.float32))
    found = jnp.dot(
        piece[...], all_slabs(2 * (mains - ready)), preferred_element_type=jnp.float32
    )
    extended[:, :LANES] = rounded(found)
    taps = jnp.concatenate([conv_gate[:, mains * LANES :], conv_up[:, mains * LANES :]], axis=1)
    both = convolve(0, LANES, taps)
    product = silu(both) * pltpu.roll(both, LANES - rest, axis=1)
    inside = lax.broadcasted_iota(jnp.int32, product.shape, 1) < rest
    hidden[:, mains * LANES :] = jnp.where(inside, product, 0.0).astype(jnp.bfloat16)
    w.finish(0)
    for j in range(ready):
        gated(j, early[j] + pair_product(wrap(z + RING // 2, RING), j))

    wide = depth // 2
    sides_of = [pl.ds(0, wide), pl.ds(wide, wide)]
    halves = (pl.ds(0, own_rows // 2), pl.ds(own_rows // 2, own_rows // 2))
    halved, summing = post.kind(), post.kind()
    swap_in = [post.slot(), post.slot()]
    for part in (0, 1):
        for j in range(part * RING // 2, (part + 1) * RING // 2):
            end = late_blocks[j, :, len(later_blocks) * slab :].astype(jnp.float32)
            end = end.reshape(RING * half, LANES)
            inside = lax.broadcasted_iota(jnp.int32, end.shape, 1) < rest
            ends = [
                jnp.where(inside, v, 0.0).astype(jnp.bfloat16).reshape(RING, half, LANES)
                for v in (end, pltpu.roll(end, LANES - rest, axis=1))
            ]
            rhs = jnp.concatenate(
                [slabs(late_blocks, j, down_at + k) for k in range(mains)]
                + [jnp.concatenate(ends, axis=1).reshape(stripe, LANES)],
                axis=1,
            )
            found = lax.dot_general(
                hidden[...], rhs, (((1,), (1,)), ((), ())), preferred_element_type=jnp.float32
            )
            partial[:, :, j * stripe : (j + 1) * stripe] = found.astype(jnp.bfloat16).reshape(
                partial.shape[0], own_rows, stripe
            )
        for chip in range(CHIPS):
            started(
                partial.at[2 * chip + 1 - core, :, sides_of[part]],
                partner_partial.at[chip, :, sides_of[part]],
                halved,
                swap_in[part],
                partner,
            )

    ends_in = post.slot()

    def give(src, slot, part, chip):
        there = landed.at[slot, :, sides_of[part]]
        arrival = post.slot() if slot < 2 else ends_in
        return started(src, there, summing, arrival, to_chip(chip))

    got = []
    for part in (0, 1):
        cols = sides_of[part]
        swaps = partner_partial.at[:, :, cols]
        remote(swaps, swaps, halved, swap_in[part], partner).wait_recv()
        for chip in (far, right, left, x):
            summed[chip, :, cols] = (
                partial[2 * chip + core, :, cols].astype(jnp.float32)
                + partner_partial[chip, :, cols].astype(jnp.float32)
            ).astype(jnp.bfloat16)
        got.append(
            [
                give(summed.at[far, halves[0], cols], 0, part, right),
                give(summed.at[far, halves[1], cols], 1, part, left),
                give(summed.at[right, halves[1], cols], 2, part, right),
                give(summed.at[left, halves[0], cols], 3, part, left),
            ]
        )
    kv.drain()
    qs.drain()
    w.drain()
    remote(pieces, pieces, swapped, swapped, partner).wait_send()
    moved = piece.at[pl.ds(0, (GROUP - 1) * own_rows)]
    remote(moved, moved, spread_out, spread_out, partner).wait_send()

    def sent(turn, carry):
        result_copy(z + 1 + turn, z).wait_send()
        return carry

    lax.fori_loop(0, others, sent, 0)
    for part in (0, 1):
        cols = sides_of[part]
        for k, (toward, half) in enumerate(((right, 0), (left, 1))):
            got[part][k].wait_recv()
            passed[k, :, cols] = (
                summed[toward, halves[half], cols].astype(jnp.float32)
                + landed[k, :, cols].astype(jnp.float32)
            ).astype(jnp.bfloat16)
            give(passed.at[k, :, cols], 4 + k, part, toward)
    ending = landed.at[pl.ds(2, 4)]
    remote(ending, ending, summing, ends_in, partner).wait_recv()
    for h, (near, through) in enumerate(((3, 4), (2, 5))):
        ffn = rounded(
            summed[x, halves[h], :].astype(jnp.float32)
            + landed[near].astype(jnp.float32)
            + landed[through].astype(jnp.float32)
        )
        result[halves[h], :] = (
            middle[halves[h], :] + gain_post[...] * rms_scale(ffn)
        ).astype(jnp.bfloat16)

    remote(partner_partial, partner_partial, halved, halved, partner).wait_send()
    remote(landed, landed, summing, summing, partner).wait_send()

    @pl.when(last & (sp < shards - 1))
    def _():
        ahead.wait_send()

    @pl.when(last & (sp > 0))
    def _():
        for copy in spread:
            copy.wait_send()


def local(
    queries,
    keys,
    values,
    score_shift,
    resid,
    w_out,
    gain_mix,
    gain_pre,
    w_gate,
    w_up,
    conv_gate,
    conv_up,
    w_down,
    gain_post,
):
    span = queries.shape[0]
    own_rows, depth = resid.shape
    width = w_gate.shape[1]
    mains = width // LANES
    slab = w_gate.shape[0]
    tiles = 3 * mains + 1
    early_tiles = tiles // 4 * 2
    vmem = pl.BlockSpec(memory_space=pltpu.VMEM)
    hbm = pl.BlockSpec(memory_space=pltpu.HBM)
    bf16, f32 = jnp.bfloat16, jnp.float32
    return pl.pallas_call(
        layer_kernel,
        out_shape=jax.ShapeDtypeStruct((own_rows, depth), bf16),
        in_specs=[hbm] * 14,
        out_specs=vmem,
        scratch_shapes=[
            pltpu.SMEM((1,), f32),
            pltpu.VMEM((1, depth), f32),
            pltpu.VMEM((1, depth), f32),
            pltpu.VMEM((1, depth), f32),
            pltpu.VMEM(conv_gate.shape, f32),
            pltpu.VMEM(conv_up.shape, f32),
            pltpu.VMEM((RING, HEAD_DIM, span), bf16),
            pltpu.VMEM((span, LANES), bf16),
            pltpu.VMEM((RING, 2 * HEAD_DIM, span), bf16),
            pltpu.VMEM((slab, width), bf16),
            pltpu.VMEM((slab, width), bf16),
            pltpu.VMEM((slab, width), bf16),
            pltpu.VMEM((RING, RING, early_tiles * slab, LANES), bf16),
            pltpu.VMEM((RING, RING, (tiles - early_tiles) * slab + slab // 2, LANES), bf16),
            pltpu.VMEM((own_rows, depth), bf16),
            pltpu.VMEM(w_out.shape, bf16),
            pltpu.VMEM((span, span), bf16),
            pltpu.VMEM((span, LANES), f32),
            pltpu.VMEM((span, LANES), f32),
            pltpu.VMEM((span, LANES), bf16),
            pltpu.VMEM((RING, HEAD_DIM + HEAD_DIM // 4, span), bf16),
            pltpu.VMEM((RING, HEAD_DIM + HEAD_DIM // 4, span), bf16),
            pltpu.VMEM((2 * HEAD_DIM, span), f32),
            pltpu.VMEM((GROUP, own_rows, LANES), bf16),
            pltpu.VMEM((HALO + span, depth), bf16),
            pltpu.VMEM((own_rows, depth), f32),
            pltpu.VMEM((KERNEL - 1, depth), f32),
            pltpu.VMEM((KERNEL - 1, depth), f32),
            pltpu.VMEM((HALO + span, 2 * LANES), f32),
            pltpu.VMEM((span, (mains + 1) * LANES), bf16),
            pltpu.VMEM((GROUP, own_rows, depth), bf16),
            pltpu.VMEM((CHIPS, own_rows, depth), bf16),
            pltpu.VMEM((CHIPS, own_rows, depth), bf16),
            pltpu.VMEM((6, own_rows // 2, depth), bf16),
            pltpu.VMEM((2, own_rows // 2, depth), bf16),
            pltpu.SemaphoreType.DMA((KINDS,)),
            pltpu.SemaphoreType.DMA((ARRIVALS,)),
            pltpu.SemaphoreType.DMA((LOADS,)),
            pltpu.SemaphoreType.DMA((GROUP + 1,)),
            pltpu.SemaphoreType.DMA((RING,)),
            pltpu.SemaphoreType.DMA((RING,)),
            pltpu.SemaphoreType.DMA((RING * RING // 2,)),
            pltpu.VMEM((early_tiles // 2, HALO + span, 2 * LANES), f32),
        ],
        compiler_params=pltpu.CompilerParams(
            collective_id=0, has_side_effects=True, vmem_limit_bytes=67_043_328
        ),
        name="layer",
    )(
        score_shift,
        gain_mix[None],
        gain_pre[None],
        gain_post[None],
        conv_gate,
        conv_up,
        queries.T,
        keys.T,
        values.T,
        w_gate,
        w_up,
        w_down.T,
        resid,
        w_out,
    )


def solution(mesh):
    in_specs = (
        P("sp", "tp"),
        P("sp", "tp"),
        P("sp", "tp"),
        P("tp"),
        P(("sp", "tp"), None),
        P(),
        P(),
        P(),
        P("sp", "tp"),
        P("sp", "tp"),
        P(None, "tp"),
        P(None, "tp"),
        P("tp", "sp"),
        P(),
    )
    out_specs = P(("sp", "tp"), None)
    return jax.shard_map(local, mesh=mesh, in_specs=in_specs, out_specs=out_specs, check_vma=False)
```
